512 devices in a mesh: sp: 32 (over z, x), dp: 16 (over y, core).
Axes of the slice: x: 4, y: 8, z: 8, core: 2. Of those that a mesh axis runs over, the one named last changes fastest.
Arguments:
- inputs: bfloat16 [16, 4096, 2048], P('dp', 'sp'), may hold values from -6 to 6
- w_key: bfloat16 [2048, 256], P('dp')
- w_value: bfloat16 [2048, 256], P('dp'), may hold values from -0.125 to 0.125
- queries: bfloat16 [16, 4096, 2048], P('dp', 'sp')
- cotangent: bfloat16 [16, 4096, 2048], P('dp', 'sp'), may hold values from -6 to 6
- cum_gate: float32 [16, 32, 4096], P('dp', 'sp'), as said below
Outputs:
- grad_input: bfloat16 [16, 4096, 2048], P('dp', 'sp')
- grad_queries: bfloat16 [16, 4096, 2048], P('dp', 'sp')
- grad_cum: float32 [16, 32, 4096], P('dp', 'sp')
- grad_w_key: float32 [2048, 256], P('dp')
- grad_w_value: float32 [2048, 256], P('dp')
The draws below stay inside these ranges and needn't reach their ends.
Inputs may be any that keep to these rules, and one draw needn't show every extreme that they name: Along each sequence cum_gate never rises, and it is at most zero.
All inputs are finite; a program needn't handle non-finite values.
Results may differ from the reference program's by a relative error of at most 0.023.
Values may be sent and summed in bfloat16 or wider, within the bound.
No kernel may reach another device: no remote copies, remote signals or barrier semaphores. Data moves between devices by JAX's collectives and lax.ppermute only.
A program may use at most 128 MiB of HBM per device.

```python
import jax
import jax.numpy as jnp
from jax import lax

D = 2048
QUERY_HEADS_TOTAL = 32
HD = 64
KVH = 4
POS_DEV = 128
SEQUENCE_LENGTH = 4096
SEQUENCE_COUNT = 16


def shared_inputs(key):
    feature_key = jax.random.fold_in(key, 11)
    drawn = jnp.clip(jax.random.normal(feature_key, (SEQUENCE_COUNT, SEQUENCE_LENGTH, D), jnp.float32), -6.0, 6.0)
    return drawn


def shared_keyweight(key):
    drawn = jax.random.normal(jax.random.fold_in(key, 12), (D, KVH * HD), jnp.float32)
    return jnp.clip(drawn, -6.0, 6.0) * D ** (-0.5)


def draw_inputs(key, part):
    return shared_inputs(key).astype(jnp.bfloat16)


def draw_w_key(key, part):
    return shared_keyweight(key).astype(jnp.bfloat16)


def draw_queries(key, part):
    base_key = jax.random.fold_in(key, 13)
    drawn = jnp.clip(jax.random.normal(base_key, (SEQUENCE_COUNT, SEQUENCE_LENGTH, QUERY_HEADS_TOTAL * HD), jnp.float32), -6.0, 6.0)
    return drawn.astype(jnp.bfloat16)


def draw_cum_gate(key, part):
    gate_random_keys = jax.random.split(jax.random.fold_in(key, 31), 7)
    share = 0.5
    gradual_gate = jax.random.uniform(gate_random_keys[0], (1, QUERY_HEADS_TOTAL, 1), jnp.float32) < share
    total = jax.random.uniform(gate_random_keys[1], (SEQUENCE_COUNT, QUERY_HEADS_TOTAL, 1), jnp.float32, 0.3, 1.2)
    fast_span = jax.random.uniform(gate_random_keys[2], (SEQUENCE_COUNT, QUERY_HEADS_TOTAL, 1), jnp.float32, 30.0, 100.0)
    decay_rate = jnp.where(gradual_gate, total / SEQUENCE_LENGTH, 1.0 / fast_span)
    block_multiplier = jnp.exp(jax.random.uniform(gate_random_keys[3], (SEQUENCE_COUNT, QUERY_HEADS_TOTAL, SEQUENCE_LENGTH // POS_DEV), jnp.float32, -0.8, 0.8))
    block_multiplier = jnp.repeat(block_multiplier, POS_DEV, axis=2)
    coarse_gate = jax.random.uniform(gate_random_keys[4], (SEQUENCE_COUNT, QUERY_HEADS_TOTAL, SEQUENCE_LENGTH), jnp.float32, 0.5, 1.5)
    spike_position = jax.random.randint(gate_random_keys[5], (SEQUENCE_COUNT, QUERY_HEADS_TOTAL, 3), 0, SEQUENCE_LENGTH)
    spike_length = jnp.log(jax.random.uniform(gate_random_keys[6], (SEQUENCE_COUNT, QUERY_HEADS_TOTAL, 3), jnp.float32, 0.55, 0.8))
    spike_flags = jnp.arange(SEQUENCE_LENGTH)[None, None, None, :] == spike_position[:, :, :, None]
    spike_events = jnp.sum(jnp.where(spike_flags, spike_length[:, :, :, None], 0.0), axis=2)
    gate_logarithm = -decay_rate * block_multiplier * coarse_gate + jnp.where(gradual_gate, spike_events, 0.0)
    return jnp.cumsum(gate_logarithm, axis=2)


def steps_of(stream_key, extent, pieces, smallest, top_value):
    def one(axis_at, shards_of):
        heights = jax.random.uniform(jax.random.fold_in(jax.random.fold_in(stream_key, 6), axis_at), (shards_of,), jnp.float32, smallest / len(pieces), top_value / len(pieces))
        return jnp.repeat(jnp.exp(heights), extent[axis_at] // shards_of).reshape((-1,) + (1,) * (len(extent) - axis_at - 1))

    level = one(*pieces[0])
    for cut in pieces[1:]:
        level = level * one(*cut)
    return level


def centred(stream_key, dims, width, most, shards=(), held_as=jnp.bfloat16):
    values = width * jax.random.normal(stream_key, dims, jnp.float32)
    if shards:
        values = values * steps_of(stream_key, dims, shards, -0.22, 0.18)
    return jnp.clip(values, -most, most).astype(held_as)


def setup_inputs(seed: int = 0) -> dict:
    streams_of = jax.random.split(jax.random.key(seed), 7)
    return {
        "inputs": draw_inputs(jax.random.fold_in(streams_of[6], 71), 0),
        "w_key": draw_w_key(jax.random.fold_in(streams_of[6], 71), 0),
        "w_value": centred(streams_of[2], (D, KVH * HD), D ** -0.5, 0.125, ((0, 16),)),
        "queries": draw_queries(jax.random.fold_in(streams_of[6], 71), 0),
        "cotangent": centred(streams_of[4], (SEQUENCE_COUNT, SEQUENCE_LENGTH, QUERY_HEADS_TOTAL * HD), 1.0, 6.0, ((0, 16), (1, 32))),
        "cum_gate": draw_cum_gate(jax.random.fold_in(streams_of[6], 71), 0),
    }


def head_backward(item_parts):
    query_rows, key_rows, value_rows, grad_rows, cum_rows = item_parts
    seq_length = query_rows.shape[0]
    score_scale = HD ** -0.5
    scores = jnp.dot(query_rows, key_rows.T, preferred_element_type=jnp.float32) * score_scale
    scores = scores + cum_rows[:, None] - cum_rows[None, :]
    later = jnp.arange(seq_length)[None, :] > jnp.arange(seq_length)[:, None]
    scores = jnp.where(later, -jnp.inf, scores)
    row_max = jnp.max(scores, axis=1, keepdims=True)
    exp_scores = jnp.exp(scores - row_max)
    probs = exp_scores / jnp.sum(exp_scores, axis=1, keepdims=True)
    probs_low = probs.astype(jnp.bfloat16)
    outputs = jnp.dot(probs_low, value_rows, preferred_element_type=jnp.float32)
    row_dot = jnp.sum(grad_rows.astype(jnp.float32) * outputs, axis=1)
    grad_probs = jnp.dot(grad_rows, value_rows.T, preferred_element_type=jnp.float32)
    grad_scores = probs * (grad_probs - row_dot[:, None])
    grad_low = grad_scores.astype(jnp.bfloat16)
    grad_query = (jnp.dot(grad_low, key_rows, preferred_element_type=jnp.float32) * score_scale).astype(jnp.bfloat16)
    key_term = (jnp.dot(grad_low.T, query_rows, preferred_element_type=jnp.float32) * score_scale).astype(jnp.bfloat16)
    value_term = jnp.dot(probs_low.T, grad_rows, preferred_element_type=jnp.float32).astype(jnp.bfloat16)
    grad_cum = jnp.sum(grad_scores, axis=1) - jnp.sum(grad_scores, axis=0)
    return grad_query, key_term, value_term, grad_cum


def reference(inputs, w_key, w_value, queries, cotangent, cum_gate):
    seq_count, seq_length, feature_count = inputs.shape
    group_size = QUERY_HEADS_TOTAL // KVH
    flat_rows = inputs.reshape(seq_count * seq_length, feature_count)
    key_proj = jnp.dot(flat_rows, w_key, preferred_element_type=jnp.float32).astype(jnp.bfloat16)
    value_proj = jnp.dot(flat_rows, w_value, preferred_element_type=jnp.float32).astype(jnp.bfloat16)

    def spread(projected):
        split_heads = projected.reshape(seq_count, seq_length, KVH, HD)
        repeated = jnp.repeat(split_heads, group_size, axis=2)
        return repeated.transpose(0, 2, 1, 3).reshape(seq_count * QUERY_HEADS_TOTAL, seq_length, HD)

    def by_head(tensor):
        return tensor.reshape(seq_count, seq_length, QUERY_HEADS_TOTAL, HD).transpose(0, 2, 1, 3).reshape(seq_count * QUERY_HEADS_TOTAL, seq_length, HD)

    grad_query, key_term, value_term, grad_cum = lax.map(
        head_backward,
        (by_head(queries), spread(key_proj), spread(value_proj), by_head(cotangent),
         cum_gate.reshape(seq_count * QUERY_HEADS_TOTAL, seq_length)))

    def to_tokens(tensor):
        return tensor.reshape(seq_count, QUERY_HEADS_TOTAL, seq_length, HD).transpose(0, 2, 1, 3)

    grad_queries = to_tokens(grad_query).reshape(seq_count, seq_length, QUERY_HEADS_TOTAL * HD)

    def group_sum(tensor):
        grouped = to_tokens(tensor).reshape(seq_count * seq_length, KVH, group_size, HD)
        return jnp.sum(grouped.astype(jnp.float32), axis=2).astype(jnp.bfloat16).reshape(seq_count * seq_length, KVH * HD)

    grad_keys = group_sum(key_term)
    grad_values = group_sum(value_term)
    grad_input = (jnp.dot(grad_keys, w_key.T, preferred_element_type=jnp.float32)
                  + jnp.dot(grad_values, w_value.T, preferred_element_type=jnp.float32)).astype(jnp.bfloat16)
    grad_w_key = jnp.dot(flat_rows.T, grad_keys, preferred_element_type=jnp.float32)
    grad_w_value = jnp.dot(flat_rows.T, grad_values, preferred_element_type=jnp.float32)
    return (grad_input.reshape(seq_count, seq_length, feature_count), grad_queries,
            grad_cum.reshape(seq_count, QUERY_HEADS_TOTAL, seq_length), grad_w_key, grad_w_value)
```

```python
import functools

import jax
import jax.numpy as jnp
from jax import lax
from jax.experimental import pallas as pl
from jax.experimental.pallas import tpu as pltpu
from jax.sharding import Mesh
from jax.sharding import PartitionSpec as P


HD = 64
LANES = 128
LOG2E = 1.4426950408889634
BLOCK = 512
ONES = HD + 16
SP = ("zg", "zp", "x")
GROUP = ("zp", "x")
bf16 = jnp.bfloat16
f32 = jnp.float32
VMEM = pltpu.VMEM


def dot(a, b, ca, cb):
    return lax.dot_general(a, b, (((ca,), (cb,)), ((), ())), preferred_element_type=f32)


def low_half(rows):
    return lax.broadcasted_iota(jnp.int32, (rows, LANES), 1) < HD


def merge_pair(a, b):
    low = low_half(a.shape[0])
    return jnp.where(low, a, pltpu.roll(b, HD, 1)), jnp.where(low, pltpu.roll(a, HD, 1), b)


def pieces(value):
    first = value.astype(bf16).astype(f32)
    rest = value - first
    second = rest.astype(bf16).astype(f32)
    third = (rest - second).astype(bf16).astype(f32)
    return first, second, third


def call(kernel, out_shapes, *args, scratch=(), vmem=60):
    many = isinstance(out_shapes, tuple)
    specs = pl.BlockSpec(memory_space=VMEM)
    return pl.pallas_call(
        kernel,
        out_shape=out_shapes,
        in_specs=[
            pl.BlockSpec(memory_space=pltpu.SMEM) if arg.dtype == jnp.int32 else specs
            for arg in args
        ],
        out_specs=(specs,) * len(out_shapes) if many else specs,
        scratch_shapes=scratch,
        compiler_params=pltpu.CompilerParams(vmem_limit_bytes=vmem * 1024 * 1024),
    )(*args)


def shape(dims, dtype=bf16):
    return jax.ShapeDtypeStruct(dims, dtype)


def pack_weights_kernel(key_ref, value_ref, out_ref):
    for pair in range(key_ref.shape[1] // LANES):
        at = slice(pair * LANES, (pair + 1) * LANES)
        first, second = merge_pair(key_ref[:, at].astype(f32), value_ref[:, at].astype(f32))
        out_ref[:, 2 * pair * LANES : (2 * pair + 1) * LANES] = first.astype(bf16)
        out_ref[:, (2 * pair + 1) * LANES : (2 * pair + 2) * LANES] = second.astype(bf16)


def pack_queries_kernel(query_ref, grad_ref, out_ref):
    for pair in range(query_ref.shape[1] // LANES):
        at = slice(pair * LANES, (pair + 1) * LANES)
        first, second = merge_pair(query_ref[:, at].astype(f32), grad_ref[:, at].astype(f32))
        out_ref[2 * pair] = first.astype(bf16)
        out_ref[2 * pair + 1] = second.astype(bf16)


def project_kernel(rows_ref, weight_ref, out_ref, *, group):
    projected = dot(rows_ref[...], weight_ref[...], 1, 0).astype(bf16)
    for head in range(out_ref.shape[0]):
        g = head // group
        out_ref[head] = projected[:, g * LANES : (g + 1) * LANES]


def attend_kernel(
    x_ref, kv_ref, cum_ref, dq_ref, dkv_ref, gcum_ref,
    qa_ref, ka_ref, kn_ref, s_ref, dp_ref, xt_ref, dkt_ref, dvt_ref, rows_ref, acc_ref,
    *, blk, seq, members,
):
    count = seq // blk
    scale = HD**-0.5
    lane = lax.broadcasted_iota(jnp.int32, (blk, LANES), 1)
    low = lane < HD
    row_id = lax.broadcasted_iota(jnp.int32, (LANES, blk), 0)

    def prepare(i, _):
        at = pl.ds(pl.multiple_of(i * blk, blk), blk)
        x = x_ref[at, :].astype(f32)
        kv = kv_ref[at, :].astype(f32)
        c1, c2, c3 = pieces(jnp.broadcast_to(cum_ref[:, at] * LOG2E, (LANES, blk)))
        one = jnp.ones_like(c1)

        def extra(values):
            total = jnp.zeros_like(c1)
            for k, value in enumerate(values):
                total = jnp.where(row_id == HD + k, value, total)
            return total.T

        q1, q2, q3 = pieces(x * (LOG2E * scale))
        qa_ref[at, 0:LANES] = jnp.where(low, q1, pltpu.roll(q2, HD, 1)).astype(bf16)
        qa_ref[at, LANES:] = jnp.where(low, q3, extra((c1, c2, c3, one, one, one))).astype(bf16)
        ka_ref[at, 0:LANES] = jnp.where(low, kv, pltpu.roll(kv, HD, 1)).astype(bf16)
        ka_ref[at, LANES:] = jnp.where(low, kv, extra((one, one, one, -c1, -c2, -c3))).astype(bf16)
        kn_ref[at, :] = jnp.where(low, kv, jnp.where(lane == HD, 1.0, 0.0)).astype(bf16)
        xt = x.T
        ones_row = jnp.where(row_id == HD, 1.0, 0.0)
        xt_ref[0:ONES, at] = jnp.where(row_id < HD, xt, ones_row)[0:ONES].astype(bf16)
        xt_ref[ONES:, at] = xt[HD:].astype(bf16)
        dkt_ref[:, at] = jnp.zeros((ONES, blk), f32)
        dvt_ref[:, at] = jnp.zeros((HD, blk), f32)
        return 0

    lax.fori_loop(0, count, prepare, 0)

    def fold(block, op):
        result = block[:, 0:LANES]
        for k in range(1, blk // LANES):
            result = op(result, block[:, k * LANES : (k + 1) * LANES])
        return result

    def query_block(i, _):
        rows = pl.ds(pl.multiple_of(i * blk, blk), blk)
        qa = qa_ref[rows, :]
        x = x_ref[rows, :]
        grad = jnp.where(low, jnp.zeros_like(x), x)

        def score(j):
            at = pl.ds(pl.multiple_of(j * blk, blk), blk)
            scores = dot(qa, ka_ref[at, :], 1, 1)
            dp_ref[:, at] = dot(grad, kv_ref[at, :], 1, 1)
            return scores, at

        def full_block(j, best):
            scores, at = score(j)
            s_ref[:, at] = scores
            return jnp.maximum(best, fold(scores, jnp.maximum))

        scores, at = score(i)
        sub = lax.broadcasted_iota(jnp.int32, (blk, blk), 0)
        col = lax.broadcasted_iota(jnp.int32, (blk, blk), 1)
        scores = jnp.where(col <= sub, scores, -jnp.inf)
        s_ref[:, at] = scores
        best = lax.fori_loop(0, i, full_block, fold(scores, jnp.maximum))
        best = jnp.max(best, axis=1, keepdims=True)

        def exponentials(j, carry):
            total, weighted = carry
            at = pl.ds(pl.multiple_of(j * blk, blk), blk)
            e = jnp.exp2(s_ref[:, at] - best)
            s_ref[:, at] = e
            return total + fold(e, jnp.add), weighted + fold(e * dp_ref[:, at], jnp.add)

        zero = jnp.zeros((blk, LANES), f32)
        total, weighted = lax.fori_loop(0, i + 1, exponentials, (zero, zero))
        inverse = 1.0 / jnp.sum(total, axis=1, keepdims=True)
        row_dot = jnp.sum(weighted, axis=1, keepdims=True) * inverse
        acc_ref[...] = zero

        def gradients(j, _):
            at = pl.ds(pl.multiple_of(j * blk, blk), blk)
            probs = s_ref[:, at] * inverse
            grad_low = (probs * (dp_ref[:, at] - row_dot)).astype(bf16)
            probs_low = probs.astype(bf16)
            acc_ref[...] += dot(grad_low, kn_ref[at, :], 1, 0)
            dkt_ref[:, at] += dot(xt_ref[0:ONES, rows], grad_low, 1, 0)
            dvt_ref[:, at] += dot(xt_ref[ONES:, rows], probs_low, 1, 0)
            return 0

        lax.fori_loop(0, i + 1, gradients, 0)
        dq = acc_ref[...]
        rows_ref[:, rows] = dq.T[HD : HD + 8]
        dq = dq * scale
        for b in range(blk // LANES):
            top = dq[b * LANES : b * LANES + HD]
            bottom = dq[b * LANES + HD : (b + 1) * LANES]
            packed = jnp.where(low[0:HD], top, pltpu.roll(bottom, HD, 1))
            dq_ref[i * (blk // LANES) + b] = packed.astype(bf16)
        return 0

    lax.fori_loop(0, count, query_block, 0)
    for b in range(seq // LANES):
        at = slice(b * LANES, (b + 1) * LANES)
        dkv_ref[b % members, b // members, 0:HD, :] = (dkt_ref[0:HD, at] * scale).astype(bf16)
        dkv_ref[b % members, b // members, HD:, :] = dvt_ref[:, at].astype(bf16)
    gcum_ref[...] = rows_ref[0:1, :] - dkt_ref[HD : HD + 1, :]


def attend(x, kv, cum, members):
    seq = x.shape[0]
    owners = seq // LANES
    return call(
        functools.partial(attend_kernel, blk=BLOCK, seq=seq, members=members),
        (
            shape((owners, HD, LANES)),
            shape((members, owners // members, LANES, LANES)),
            shape((1, seq), f32),
        ),
        x, kv, cum,
        scratch=[
            VMEM((seq, 2 * LANES), bf16),
            VMEM((seq, 2 * LANES), bf16),
            VMEM((seq, LANES), bf16),
            VMEM((BLOCK, seq), f32),
            VMEM((BLOCK, seq), f32),
            VMEM((ONES + HD, seq), bf16),
            VMEM((ONES, seq), f32),
            VMEM((HD, seq), f32),
            VMEM((8, seq), f32),
            VMEM((BLOCK, LANES), f32),
        ],
    )


def group_sum_kernel(me_ref, terms_ref, *refs):
    owners = terms_ref.shape[1]
    rows_refs, sums_refs, part_ref = refs[:owners], refs[owners : 2 * owners], refs[2 * owners]
    part = None
    for k in range(owners):
        owner = lax.rem(me_ref[0] + k, owners)
        total = terms_ref[0, owner].astype(f32)
        for member in range(1, terms_ref.shape[0]):
            total = total + terms_ref[member, owner].astype(f32)
        low = total.astype(bf16)
        sums_refs[k][...] = low
        product = dot(low, rows_refs[(owners - k) % owners][...], 1, 0)
        part = product if part is None else part + product
    for chunk in range(part_ref.shape[0]):
        part_ref[chunk] = part[:, chunk * LANES : (chunk + 1) * LANES].astype(bf16)


def unpack_queries_kernel(packed_ref, out_ref):
    for pair in range(packed_ref.shape[0] // 2):
        top, bottom = merge_pair(
            packed_ref[2 * pair].astype(f32), packed_ref[2 * pair + 1].astype(f32)
        )
        at = slice(pair * LANES, (pair + 1) * LANES)
        out_ref[0:HD, at] = top.astype(bf16)
        out_ref[HD:, at] = bottom.astype(bf16)


def grad_input_kernel(me_ref, weight_ref, *refs):
    sums_refs, out_ref = refs[:-1], refs[-1]
    groups = len(sums_refs)
    total = None
    for k in range(groups):
        g = lax.rem(me_ref[0] + groups - k, groups)
        columns = pl.ds(pl.multiple_of(g * LANES, LANES), LANES)
        product = dot(sums_refs[k][...], weight_ref[:, columns], 0, 1)
        total = product if total is None else total + product
    out_ref[...] = total.astype(bf16)


def sum_parts_kernel(parts_ref, out_ref):
    total = parts_ref[0].astype(f32)
    for k in range(1, parts_ref.shape[0]):
        total = total + parts_ref[k].astype(f32)
    out_ref[...] = total.astype(bf16)


def sum_ring_kernel(me_ref, *refs):
    parts, out_ref, held_ref = refs[:-2], refs[-2], refs[-1]
    count = len(parts)
    for k in range(count):
        held_ref[lax.rem(me_ref[0] + count - k, count)] = parts[k][...].astype(f32)
    total = held_ref[0]
    for k in range(1, count):
        total = total + held_ref[k]
    out_ref[...] = total.astype(bf16)


def finish_kernel(me_ref, *refs):
    parts, (key_ref, value_ref, held_ref) = refs[:-3], refs[-3:]
    count = len(parts)
    for k in range(count):
        held_ref[lax.rem(me_ref[0] + count - k, count)] = parts[k][...].astype(f32).T
    for pair in range(count // 2):
        at = slice(pair * LANES, (pair + 1) * LANES)
        keys, values = merge_pair(held_ref[2 * pair], held_ref[2 * pair + 1])
        key_ref[:, at] = keys
        value_ref[:, at] = values


def exchange(x, axes):
    return lax.all_to_all(x, axes, split_axis=0, concat_axis=0, tiled=True)


def shift(x, axis, size, by):
    return lax.ppermute(x, axis, [(k, (k + by) % size) for k in range(size)])


def per_device(inputs, w_key, w_value, queries, cotangent, cum_gate, **sizes):
    return program(inputs, w_key, w_value, queries, cotangent, cum_gate, **sizes)


def program(inputs, w_key, w_value, queries, cotangent, cum_gate, *, heads, dp, zg, zp, xs):
    _, positions, features = inputs.shape
    kv_width = w_key.shape[1]
    kv_heads = kv_width // HD
    owners, members = zg, zp * xs
    rows = inputs.reshape(positions, features)
    width = 2 * kv_width
    block = shape((LANES, LANES))
    me = {axis: lax.axis_index(axis).astype(jnp.int32).reshape(1) for axis in SP}

    weight = call(pack_weights_kernel, shape((w_key.shape[0], width)), w_key, w_value)
    weight = lax.all_gather(weight, "dp", axis=0, tiled=True)
    packed = call(
        pack_queries_kernel, shape((heads, positions, LANES)),
        queries.reshape(positions, -1), cotangent.reshape(positions, -1),
    )
    head_rows = exchange(packed, SP).reshape(heads * positions, LANES)
    projected = call(
        functools.partial(project_kernel, group=heads // kv_heads),
        shape((heads, positions, LANES)), rows, weight,
    )
    head_kv = exchange(projected, SP).reshape(heads * positions, LANES)
    head_kv, late_rows = lax.optimization_barrier((head_kv, rows))
    near_rows = [late_rows] + [shift(late_rows, "zg", zg, k) for k in range(1, zg)]

    dq, dkv, grad_cum = attend(head_rows, head_kv, cum_gate[0], members)
    terms = exchange(dkv, GROUP)
    *sums, part = call(
        group_sum_kernel,
        (*[shape((LANES, positions))] * owners, shape((dp, LANES, LANES))),
        me["zg"], terms, *near_rows,
    )
    parts = exchange(part, "dp")
    own_sums = [sums[0]] + [shift(sums[k], "zg", zg, k) for k in range(1, zg)]
    grad_input = call(grad_input_kernel, shape((positions, features)), me["zg"], weight, *own_sums)
    summed = call(sum_parts_kernel, block, parts)
    query_parts = exchange(dq, SP)
    grad_queries = call(unpack_queries_kernel, shape((positions, features)), query_parts)

    def held(count):
        return [VMEM((count, LANES, LANES), f32)]

    along = [summed] + [shift(summed, "x", xs, k) for k in range(1, xs)]
    summed = call(sum_ring_kernel, block, me["x"], *along, scratch=held(xs))
    along = [summed] + [shift(summed, "zp", zp, k) for k in range(1, zp)]
    summed = call(sum_ring_kernel, block, me["zp"], *along, scratch=held(zp))
    along = [summed] + [shift(summed, "zg", zg, k) for k in range(1, zg)]
    half = shape((LANES, kv_width), f32)
    grad_key, grad_value = call(finish_kernel, (half, half), me["zg"], *along, scratch=held(zg))
    return grad_input[None], grad_queries[None], grad_cum[None], grad_key, grad_value


def solution(mesh):
    sizes = {"heads": mesh.shape["sp"], "dp": mesh.shape["dp"], "zg": 4, "zp": 2, "xs": 4}
    split = Mesh(
        mesh.devices.reshape(sizes["zg"], sizes["zp"], sizes["xs"], sizes["dp"]),
        ("zg", "zp", "x", "dp"),
    )
    rows = P("dp", SP, None)
    weights = P("dp", None)
    return jax.shard_map(
        functools.partial(per_device, **sizes),
        mesh=split,
        in_specs=(rows, weights, weights, rows, rows, rows),
        out_specs=(rows, rows, rows, weights, weights),
        check_vma=False,
    )
```

```python
import functools

import jax
import jax.numpy as jnp
from jax import lax
from jax.experimental import pallas as pl
from jax.experimental.pallas import tpu as pltpu
from jax.sharding import Mesh
from jax.sharding import PartitionSpec as P


HD = 64
LANES = 128
LOG2E = 1.4426950408889634
BLOCK = 512
UPPER = 80
ONES = HD + 16
SP = ("zg", "zp", "x")
GROUP = ("zp", "x")
bf16 = jnp.bfloat16
f32 = jnp.float32
VMEM = pltpu.VMEM


def dot(a, b, ca, cb):
    return lax.dot_general(a, b, (((ca,), (cb,)), ((), ())), preferred_element_type=f32)


def low_half(rows):
    return lax.broadcasted_iota(jnp.int32, (rows, LANES), 1) < HD


def merge_pair(a, b):
    low = low_half(a.shape[0])
    return jnp.where(low, a, pltpu.roll(b, HD, 1)), jnp.where(low, pltpu.roll(a, HD, 1), b)


def pieces(value):
    first = value.astype(bf16).astype(f32)
    rest = value - first
    second = rest.astype(bf16).astype(f32)
    third = (rest - second).astype(bf16).astype(f32)
    return first, second, third


def call(kernel, out_shapes, *args, scratch=(), vmem=60):
    many = isinstance(out_shapes, tuple)
    specs = pl.BlockSpec(memory_space=VMEM)
    return pl.pallas_call(
        kernel,
        out_shape=out_shapes,
        in_specs=[
            pl.BlockSpec(memory_space=pltpu.SMEM) if arg.dtype == jnp.int32 else specs
            for arg in args
        ],
        out_specs=(specs,) * len(out_shapes) if many else specs,
        scratch_shapes=scratch,
        compiler_params=pltpu.CompilerParams(vmem_limit_bytes=vmem * 1024 * 1024),
    )(*args)


def shape(dims, dtype=bf16):
    return jax.ShapeDtypeStruct(dims, dtype)


def pack_weights_kernel(key_ref, value_ref, out_ref):
    for pair in range(key_ref.shape[1] // LANES):
        at = slice(pair * LANES, (pair + 1) * LANES)
        first, second = merge_pair(key_ref[:, at].astype(f32), value_ref[:, at].astype(f32))
        out_ref[:, 2 * pair * LANES : (2 * pair + 1) * LANES] = first.astype(bf16)
        out_ref[:, (2 * pair + 1) * LANES : (2 * pair + 2) * LANES] = second.astype(bf16)


def pack_queries_kernel(query_ref, grad_ref, out_ref):
    for pair in range(query_ref.shape[1] // LANES):
        at = slice(pair * LANES, (pair + 1) * LANES)
        first, second = merge_pair(query_ref[:, at].astype(f32), grad_ref[:, at].astype(f32))
        out_ref[2 * pair] = first.astype(bf16)
        out_ref[2 * pair + 1] = second.astype(bf16)


def project_kernel(rows_ref, first_ref, second_ref, out_ref, weight_ref):
    depth = weight_ref.shape[0] // LANES
    upper, lower = first_ref.shape[0] // depth, second_ref.shape[0] // depth
    for k in range(depth):
        weight_ref[k * LANES : k * LANES + upper] = first_ref[k * upper : (k + 1) * upper]
        weight_ref[k * LANES + upper : (k + 1) * LANES] = second_ref[k * lower : (k + 1) * lower]
    projected = dot(rows_ref[...], weight_ref[...], 1, 0).astype(bf16)
    for g in range(out_ref.shape[0]):
        out_ref[g] = projected[:, g * LANES : (g + 1) * LANES]


def copies_kernel(x_ref, out_ref):
    for k in range(out_ref.shape[0]):
        out_ref[k] = x_ref[...]


def attend_kernel(
    x_ref, parts_ref, cum_ref, dq_ref, dkv_ref, gcum_ref,
    kv_ref, qa_ref, ka_ref, kn_ref, s_ref, dp_ref, xt_ref, dkt_ref, dvt_ref, rows_ref, acc_ref,
    *, blk, seq, members,
):
    count = seq // blk
    scale = HD**-0.5
    lane = lax.broadcasted_iota(jnp.int32, (blk, LANES), 1)
    low = lane < HD
    row_id = lax.broadcasted_iota(jnp.int32, (LANES, blk), 0)

    def prepare(i, _):
        at = pl.ds(pl.multiple_of(i * blk, blk), blk)
        x = x_ref[at, :].astype(f32)
        for b in range(blk // LANES):
            owner = i * (blk // LANES) + b
            block = parts_ref[lax.rem(owner, members), lax.div(owner, members)]
            kv_ref[pl.ds(pl.multiple_of(owner * LANES, LANES), LANES), :] = block
        kv = kv_ref[at, :].astype(f32)
        c1, c2, c3 = pieces(jnp.broadcast_to(cum_ref[:, at] * LOG2E, (LANES, blk)))
        one = jnp.ones_like(c1)

        def extra(values):
            total = jnp.zeros_like(c1)
            for k, value in enumerate(values):
                total = jnp.where(row_id == HD + k, value, total)
            return total.T

        q1, q2, q3 = pieces(x * (LOG2E * scale))
        qa_ref[at, 0:LANES] = jnp.where(low, q1, pltpu.roll(q2, HD, 1)).astype(bf16)
        qa_ref[at, LANES:] = jnp.where(low, q3, extra((c1, c2, c3, one, one, one))).astype(bf16)
        ka_ref[at, 0:LANES] = jnp.where(low, kv, pltpu.roll(kv, HD, 1)).astype(bf16)
        ka_ref[at, LANES:] = jnp.where(low, kv, extra((one, one, one, -c1, -c2, -c3))).astype(bf16)
        kn_ref[at, :] = jnp.where(low, kv, jnp.where(lane == HD, 1.0, 0.0)).astype(bf16)
        xt = x.T
        ones_row = jnp.where(row_id == HD, 1.0, 0.0)
        xt_ref[0:ONES, at] = jnp.where(row_id < HD, xt, ones_row)[0:ONES].astype(bf16)
        xt_ref[ONES:, at] = xt[HD:].astype(bf16)
        dkt_ref[:, at] = jnp.zeros((ONES, blk), f32)
        dvt_ref[:, at] = jnp.zeros((HD, blk), f32)
        return 0

    lax.fori_loop(0, count, prepare, 0)

    def fold(block, op):
        result = block[:, 0:LANES]
        for k in range(1, blk // LANES):
            result = op(result, block[:, k * LANES : (k + 1) * LANES])
        return result

    def query_block(i, _):
        rows = pl.ds(pl.multiple_of(i * blk, blk), blk)
        qa = qa_ref[rows, :]
        x = x_ref[rows, :]
        grad = jnp.where(low, jnp.zeros_like(x), x)

        def score(j):
            at = pl.ds(pl.multiple_of(j * blk, blk), blk)
            scores = dot(qa, ka_ref[at, :], 1, 1)
            dp_ref[:, at] = dot(grad, kv_ref[at, :], 1, 1)
            return scores, at

        def full_block(j, best):
            scores, at = score(j)
            s_ref[:, at] = scores
            return jnp.maximum(best, fold(scores, jnp.maximum))

        scores, at = score(i)
        sub = lax.broadcasted_iota(jnp.int32, (blk, blk), 0)
        col = lax.broadcasted_iota(jnp.int32, (blk, blk), 1)
        scores = jnp.where(col <= sub, scores, -jnp.inf)
        s_ref[:, at] = scores
        best = lax.fori_loop(0, i, full_block, fold(scores, jnp.maximum))
        best = jnp.max(best, axis=1, keepdims=True)

        def exponentials(j, carry):
            total, weighted = carry
            at = pl.ds(pl.multiple_of(j * blk, blk), blk)
            e = jnp.exp2(s_ref[:, at] - best)
            s_ref[:, at] = e
            return total + fold(e, jnp.add), weighted + fold(e * dp_ref[:, at], jnp.add)

        zero = jnp.zeros((blk, LANES), f32)
        total, weighted = lax.fori_loop(0, i + 1, exponentials, (zero, zero))
        inverse = 1.0 / jnp.sum(total, axis=1, keepdims=True)
        row_dot = jnp.sum(weighted, axis=1, keepdims=True) * inverse
        acc_ref[...] = zero

        def gradients(j, _):
            at = pl.ds(pl.multiple_of(j * blk, blk), blk)
            probs = s_ref[:, at] * inverse
            grad_low = (probs * (dp_ref[:, at] - row_dot)).astype(bf16)
            probs_low = probs.astype(bf16)
            acc_ref[...] += dot(grad_low, kn_ref[at, :], 1, 0)
            dkt_ref[:, at] += dot(xt_ref[0:ONES, rows], grad_low, 1, 0)
            dvt_ref[:, at] += dot(xt_ref[ONES:, rows], probs_low, 1, 0)
            return 0

        lax.fori_loop(0, i + 1, gradients, 0)
        dq = acc_ref[...]
        rows_ref[:, rows] = dq.T[HD : HD + 8]
        dq = dq * scale
        for b in range(blk // LANES):
            top = dq[b * LANES : b * LANES + HD]
            bottom = dq[b * LANES + HD : (b + 1) * LANES]
            packed = jnp.where(low[0:HD], top, pltpu.roll(bottom, HD, 1))
            dq_ref[i * (blk // LANES) + b] = packed.astype(bf16)
        return 0

    lax.fori_loop(0, count, query_block, 0)
    for b in range(seq // LANES):
        at = slice(b * LANES, (b + 1) * LANES)
        dkv_ref[b % members, b // members, 0:HD, :] = (dkt_ref[0:HD, at] * scale).astype(bf16)
        dkv_ref[b % members, b // members, HD:, :] = dvt_ref[:, at].astype(bf16)
    gcum_ref[...] = rows_ref[0:1, :] - dkt_ref[HD : HD + 1, :]


def attend(x, parts, cum):
    members = parts.shape[0]
    seq = x.shape[0]
    owners = seq // LANES
    return call(
        functools.partial(attend_kernel, blk=BLOCK, seq=seq, members=members),
        (
            shape((owners, HD, LANES)),
            shape((members, owners // members, LANES, LANES)),
            shape((1, seq), f32),
        ),
        x, parts, cum,
        scratch=[
            VMEM((seq, LANES), bf16),
            VMEM((seq, 2 * LANES), bf16),
            VMEM((seq, 2 * LANES), bf16),
            VMEM((seq, LANES), bf16),
            VMEM((BLOCK, seq), f32),
            VMEM((BLOCK, seq), f32),
            VMEM((ONES + HD, seq), bf16),
            VMEM((ONES, seq), f32),
            VMEM((HD, seq), f32),
            VMEM((8, seq), f32),
            VMEM((BLOCK, LANES), f32),
        ],
    )


def group_sum_kernel(me_ref, terms_ref, rows_ref, *refs):
    owners = terms_ref.shape[1]
    sums_refs, part_ref = refs[:owners], refs[owners]
    part = None
    for k in range(owners):
        owner = lax.rem(me_ref[0] + k, owners)
        total = terms_ref[0, owner].astype(f32)
        for member in range(1, terms_ref.shape[0]):
            total = total + terms_ref[member, owner].astype(f32)
        low = total.astype(bf16)
        sums_refs[k][...] = low
        product = dot(low, rows_ref[owner], 1, 0)
        part = product if part is None else part + product
    for chunk in range(part_ref.shape[0]):
        part_ref[chunk] = part[:, chunk * LANES : (chunk + 1) * LANES].astype(bf16)


def unpack_queries_kernel(packed_ref, out_ref):
    for pair in range(packed_ref.shape[0] // 2):
        top, bottom = merge_pair(
            packed_ref[2 * pair].astype(f32), packed_ref[2 * pair + 1].astype(f32)
        )
        at = slice(pair * LANES, (pair + 1) * LANES)
        out_ref[0:HD, at] = top.astype(bf16)
        out_ref[HD:, at] = bottom.astype(bf16)


def grad_input_kernel(me_ref, weight_ref, *refs):
    sums_refs, out_ref = refs[:-1], refs[-1]
    groups = len(sums_refs)
    total = None
    for k in range(groups):
        g = lax.rem(me_ref[0] + groups - k, groups)
        columns = pl.ds(pl.multiple_of(g * LANES, LANES), LANES)
        product = dot(sums_refs[k][...], weight_ref[:, columns], 0, 1)
        total = product if total is None else total + product
    out_ref[...] = total.astype(bf16)


def sum_parts_kernel(parts_ref, out_ref):
    total = parts_ref[0].astype(f32)
    for k in range(1, parts_ref.shape[0]):
        total = total + parts_ref[k].astype(f32)
    out_ref[...] = total.astype(bf16)


def finish_kernel(parts_ref, key_ref, value_ref):
    for pair in range(parts_ref.shape[0] // 2):
        at = slice(pair * LANES, (pair + 1) * LANES)
        first = parts_ref[2 * pair].astype(f32).T
        second = parts_ref[2 * pair + 1].astype(f32).T
        key_ref[:, at], value_ref[:, at] = merge_pair(first, second)


def exchange(x, axes):
    return lax.all_to_all(x, axes, split_axis=0, concat_axis=0, tiled=True)


def gather(x, axes, tiled):
    return lax.all_gather(x, axes, axis=0, tiled=tiled)


def shift(x, axis, size, by):
    return lax.ppermute(x, axis, [(k, (k + by) % size) for k in range(size)])


def per_device(inputs, w_key, w_value, queries, cotangent, cum_gate, **sizes):
    return program(inputs, w_key, w_value, queries, cotangent, cum_gate, **sizes)


def program(inputs, w_key, w_value, queries, cotangent, cum_gate, *, heads, dp, zg, zp, xs):
    _, positions, features = inputs.shape
    kv_width = w_key.shape[1]
    kv_heads = kv_width // HD
    owners, members = zg, zp * xs
    rows = inputs.reshape(positions, features)
    width = 2 * kv_width
    block = shape((LANES, LANES))
    me = lax.axis_index("zg").astype(jnp.int32).reshape(1)

    local = call(pack_weights_kernel, shape((w_key.shape[0], width)), w_key, w_value)
    first = gather(local[:UPPER], "dp", True)
    packed = call(
        pack_queries_kernel, shape((heads, positions, LANES)),
        queries.reshape(positions, -1), cotangent.reshape(positions, -1),
    )
    head_rows = exchange(packed, SP).reshape(heads * positions, LANES)
    second = gather(local[UPPER:], "dp", True)
    projected, weight = call(
        project_kernel,
        (shape((kv_heads, positions, LANES)), shape((features, width))),
        rows, first, second,
    )
    group_kv = exchange(projected, "zg")
    copies = call(copies_kernel, shape((members, *group_kv.shape)), group_kv)
    head_kv = exchange(copies, GROUP)
    head_kv, late_rows = lax.optimization_barrier((head_kv, rows))
    near_rows = gather(late_rows, "zg", False)

    dq, dkv, grad_cum = attend(head_rows, head_kv, cum_gate[0])
    terms = exchange(dkv, GROUP)
    *sums, part = call(
        group_sum_kernel,
        (*[shape((LANES, positions))] * owners, shape((dp, LANES, LANES))),
        me, terms, near_rows,
    )
    parts = exchange(part, "dp")
    own_sums = [sums[0]] + [shift(sums[k], "zg", zg, k) for k in range(1, zg)]
    grad_input = call(grad_input_kernel, shape((positions, features)), me, weight, *own_sums)
    summed = call(sum_parts_kernel, block, parts)
    query_parts = exchange(dq, SP)
    grad_queries = call(unpack_queries_kernel, shape((positions, features)), query_parts)

    along = gather(summed, GROUP, False)
    summed = call(sum_parts_kernel, block, along)
    along = gather(summed, "zg", False)
    half = shape((LANES, kv_width), f32)
    grad_key, grad_value = call(finish_kernel, (half, half), along)
    return grad_input[None], grad_queries[None], grad_cum[None], grad_key, grad_value


def solution(mesh):
    sizes = {"heads": mesh.shape["sp"], "dp": mesh.shape["dp"], "zg": 4, "zp": 2, "xs": 4}
    split = Mesh(
        mesh.devices.reshape(sizes["zg"], sizes["zp"], sizes["xs"], sizes["dp"]),
        ("zg", "zp", "x", "dp"),
    )
    rows = P("dp", SP, None)
    weights = P("dp", None)
    return jax.shard_map(
        functools.partial(per_device, **sizes),
        mesh=split,
        in_specs=(rows, weights, weights, rows, rows, rows),
        out_specs=(rows, rows, rows, weights, weights),
        check_vma=False,
    )
```

```python
import functools

import jax
import jax.numpy as jnp
from jax import lax
from jax.experimental import pallas as pl
from jax.experimental.pallas import tpu as pltpu
from jax.sharding import Mesh
from jax.sharding import PartitionSpec as P


HD = 64
LANES = 128
LOG2E = 1.4426950408889634
BLOCK = 512
ONES = HD + 16
SP = ("z", "x")
LOWEST = -3.4028235e38
bf16 = jnp.bfloat16
f32 = jnp.float32
VMEM = pltpu.VMEM


def dot(a, b, ca, cb):
    return lax.dot_general(a, b, (((ca,), (cb,)), ((), ())), preferred_element_type=f32)


def low_half(rows):
    return lax.broadcasted_iota(jnp.int32, (rows, LANES), 1) < HD


def merge_pair(a, b):
    low = low_half(a.shape[0])
    return jnp.where(low, a, pltpu.roll(b, HD, 1)), jnp.where(low, pltpu.roll(a, HD, 1), b)


def pieces(value):
    first = value.astype(bf16).astype(f32)
    rest = value - first
    second = rest.astype(bf16).astype(f32)
    third = (rest - second).astype(bf16).astype(f32)
    return first, second, third


def call(kernel, out_shapes, *args, scratch=(), vmem=60):
    many = isinstance(out_shapes, tuple)
    specs = pl.BlockSpec(memory_space=VMEM)
    return pl.pallas_call(
        kernel,
        out_shape=out_shapes,
        in_specs=[
            pl.BlockSpec(memory_space=pltpu.SMEM) if arg.dtype == jnp.int32 else specs
            for arg in args
        ],
        out_specs=(specs,) * len(out_shapes) if many else specs,
        scratch_shapes=scratch,
        compiler_params=pltpu.CompilerParams(vmem_limit_bytes=vmem * 1024 * 1024),
    )(*args)


def shape(dims, dtype=bf16):
    return jax.ShapeDtypeStruct(dims, dtype)


def pack_weights_kernel(me_ref, key_ref, value_ref, out_ref):
    at = pl.ds(pl.multiple_of(lax.div(me_ref[0], 2) * LANES, LANES), LANES)
    first, second = merge_pair(key_ref[:, at].astype(f32), value_ref[:, at].astype(f32))
    out_ref[...] = jnp.where(lax.rem(me_ref[0], 2) == 0, first, second).astype(bf16)


def pack_queries_kernel(query_ref, grad_ref, out_ref, *, members):
    heads = out_ref.shape[0]
    quads = heads // members
    for pair in range(heads // 2):
        at = slice(pair * LANES, (pair + 1) * LANES)
        blocks = merge_pair(query_ref[:, at].astype(f32), grad_ref[:, at].astype(f32))
        for k in range(2):
            head = 2 * pair + k
            out_ref[head % members * quads + head // members] = blocks[k].astype(bf16)


def project_kernel(me_ref, weight_ref, *refs):
    rows_refs, (out_ref, copies_ref) = refs[:-2], refs[-2:]
    quads = len(rows_refs)
    weight = weight_ref[...]
    for k in range(quads):
        owner = lax.rem(me_ref[0] + quads - k, quads)
        projected = dot(rows_refs[k][...], weight, 1, 0).astype(bf16)
        for member in range(out_ref.shape[0]):
            out_ref[member, owner] = projected
    for k in range(copies_ref.shape[0]):
        copies_ref[k] = weight


def attend_kernel(
    x_ref, kv_ref, cum_ref, dq_ref, dkv_ref, gcum_ref,
    qa_ref, ka_ref, kn_ref, s_ref, dp_ref, xt_ref, dkt_ref, dvt_ref, rows_ref, acc_ref, stat_ref,
    *, blk, seq,
):
    count = seq // blk
    quads = dkv_ref.shape[1]
    scale = HD**-0.5
    lane = lax.broadcasted_iota(jnp.int32, (blk, LANES), 1)
    low = lane < HD
    row_id = lax.broadcasted_iota(jnp.int32, (LANES, blk), 0)

    def span(i):
        return pl.ds(pl.multiple_of(i * blk, blk), blk)

    def prepare(i, _):
        at = span(i)
        x = x_ref[at, :].astype(f32)
        kv = kv_ref[at, :].astype(f32)
        c1, c2, c3 = pieces(jnp.broadcast_to(cum_ref[:, at] * LOG2E, (LANES, blk)))
        one = jnp.ones_like(c1)

        def extra(values):
            total = jnp.zeros_like(c1)
            for k, value in enumerate(values):
                total = jnp.where(row_id == HD + k, value, total)
            return total.T

        q1, q2, q3 = pieces(x * (LOG2E * scale))
        qa_ref[at, 0:LANES] = jnp.where(low, q1, pltpu.roll(q2, HD, 1)).astype(bf16)
        qa_ref[at, LANES:] = jnp.where(low, q3, extra((c1, c2, c3, one, one, one))).astype(bf16)
        ka_ref[at, 0:LANES] = jnp.where(low, kv, pltpu.roll(kv, HD, 1)).astype(bf16)
        ka_ref[at, LANES:] = jnp.where(low, kv, extra((one, one, one, -c1, -c2, -c3))).astype(bf16)
        kn_ref[at, :] = jnp.where(low, kv, jnp.where(lane == HD, 1.0, 0.0)).astype(bf16)
        xt = x.T
        ones_row = jnp.where(row_id == HD, 1.0, 0.0)
        xt_ref[0:ONES, at] = jnp.where(row_id < HD, xt, ones_row)[0:ONES].astype(bf16)
        xt_ref[ONES:, at] = xt[HD:].astype(bf16)
        dkt_ref[:, at] = jnp.zeros((ONES, blk), f32)
        dvt_ref[:, at] = jnp.zeros((HD, blk), f32)
        return 0

    lax.fori_loop(0, count, prepare, 0)

    def tiles(block):
        return [block[:, k * LANES : (k + 1) * LANES] for k in range(blk // LANES)]

    def query_block(i, _):
        rows = span(i)

        def score(j, diagonal):
            at = span(j)
            x = x_ref[rows, :]
            scores = dot(qa_ref[rows, :], ka_ref[at, :], 1, 1)
            if diagonal:
                sub = lax.broadcasted_iota(jnp.int32, (blk, blk), 0)
                col = lax.broadcasted_iota(jnp.int32, (blk, blk), 1)
                scores = jnp.where(col <= sub, scores, LOWEST)
            weights = dot(jnp.where(low, jnp.zeros_like(x), x), kv_ref[at, :], 1, 1)
            s_ref[:, at] = scores
            dp_ref[:, at] = weights
            return tiles(scores), tiles(weights)

        def tally(scores, weights, best):
            total = weighted = None
            for s, w in zip(scores, weights):
                e = jnp.exp2(s - best)
                total = e if total is None else total + e
                weighted = e * w if weighted is None else weighted + e * w
            return total, weighted

        scores, weights = score(i, True)
        best = functools.reduce(jnp.maximum, scores)
        stat_ref[0] = best
        stat_ref[1], stat_ref[2] = tally(scores, weights, best)

        def full_block(j, _):
            scores, weights = score(j, False)
            old = stat_ref[0]
            best = functools.reduce(jnp.maximum, scores, old)
            shrink = jnp.exp2(old - best)
            total, weighted = tally(scores, weights, best)
            stat_ref[0] = best
            stat_ref[1] = stat_ref[1] * shrink + total
            stat_ref[2] = stat_ref[2] * shrink + weighted
            return 0

        lax.fori_loop(0, i, full_block, 0)
        best = stat_ref[0]
        top = jnp.max(best, axis=1, keepdims=True)
        shrink = jnp.exp2(best - top)
        total = jnp.sum(stat_ref[1] * shrink, axis=1, keepdims=True)
        row_dot = jnp.sum(stat_ref[2] * shrink, axis=1, keepdims=True) / total
        stat_ref[0] = jnp.broadcast_to(top + jnp.log2(total), (blk, LANES))
        stat_ref[1] = jnp.broadcast_to(row_dot, (blk, LANES))
        acc_ref[...] = jnp.zeros((blk, LANES), f32)

        def gradients(j, _):
            at = span(j)
            level, row_dot = stat_ref[0], stat_ref[1]
            probs = [jnp.exp2(s - level) for s in tiles(s_ref[:, at])]
            grads = [p * (w - row_dot) for p, w in zip(probs, tiles(dp_ref[:, at]))]
            grad_low = jnp.concatenate([g.astype(bf16) for g in grads], axis=1)
            probs_low = jnp.concatenate([p.astype(bf16) for p in probs], axis=1)
            acc_ref[...] += dot(grad_low, kn_ref[at, :], 1, 0)
            dkt_ref[:, at] += dot(xt_ref[0:ONES, rows], grad_low, 1, 0)
            dvt_ref[:, at] += dot(xt_ref[ONES:, rows], probs_low, 1, 0)
            return 0

        lax.fori_loop(0, i + 1, gradients, 0)
        dq = acc_ref[...]
        rows_ref[:, rows] = dq.T[HD : HD + 8]
        dq = dq * scale
        for b in range(blk // LANES):
            upper = dq[b * LANES : b * LANES + HD]
            lower = dq[b * LANES + HD : (b + 1) * LANES]
            packed = jnp.where(low[0:HD], upper, pltpu.roll(lower, HD, 1))
            dq_ref[i * (blk // LANES) + b] = packed.astype(bf16)
        return 0

    lax.fori_loop(0, count, query_block, 0)
    for b in range(seq // LANES):
        at = slice(b * LANES, (b + 1) * LANES)
        dkv_ref[b // quads, b % quads, 0:HD, :] = (dkt_ref[0:HD, at] * scale).astype(bf16)
        dkv_ref[b // quads, b % quads, HD:, :] = dvt_ref[:, at].astype(bf16)
    gcum_ref[...] = rows_ref[0:1, :] - dkt_ref[HD : HD + 1, :]


def attend(x, kv, cum, quads):
    seq = x.shape[0]
    owners = seq // LANES
    return call(
        functools.partial(attend_kernel, blk=BLOCK, seq=seq),
        (
            shape((owners, HD, LANES)),
            shape((owners // quads, quads, LANES, LANES)),
            shape((1, seq), f32),
        ),
        x, kv, cum,
        scratch=[
            VMEM((seq, 2 * LANES), bf16),
            VMEM((seq, 2 * LANES), bf16),
            VMEM((seq, LANES), bf16),
            VMEM((BLOCK, seq), f32),
            VMEM((BLOCK, seq), f32),
            VMEM((ONES + HD, seq), bf16),
            VMEM((ONES, seq), f32),
            VMEM((HD, seq), f32),
            VMEM((8, seq), f32),
            VMEM((BLOCK, LANES), f32),
            VMEM((3, BLOCK, LANES), f32),
        ],
    )


def group_sum_kernel(me_ref, terms_ref, *refs):
    owners = terms_ref.shape[1]
    rows_refs, sums_refs, part_ref = refs[:owners], refs[owners : 2 * owners], refs[2 * owners]
    part = None
    for k in range(owners):
        owner = lax.rem(me_ref[0] + k, owners)
        total = terms_ref[0, owner].astype(f32)
        for member in range(1, terms_ref.shape[0]):
            total = total + terms_ref[member, owner].astype(f32)
        low = total.astype(bf16)
        sums_refs[k][...] = low
        product = dot(low, rows_refs[(owners - k) % owners][...], 1, 0)
        part = product if part is None else part + product
    for chunk in range(part_ref.shape[0]):
        part_ref[chunk] = part[:, chunk * LANES : (chunk + 1) * LANES].astype(bf16)


def unpack_queries_kernel(packed_ref, out_ref, *, members):
    heads = packed_ref.shape[0]
    quads = heads // members
    for pair in range(heads // 2):
        blocks = [
            packed_ref[head % members * quads + head // members].astype(f32)
            for head in (2 * pair, 2 * pair + 1)
        ]
        upper, lower = merge_pair(*blocks)
        at = slice(pair * LANES, (pair + 1) * LANES)
        out_ref[0:HD, at] = upper.astype(bf16)
        out_ref[HD:, at] = lower.astype(bf16)


def grad_input_kernel(me_ref, weight_ref, *refs):
    sums_refs, out_ref = refs[:-1], refs[-1]
    groups = len(sums_refs)
    total = None
    for k in range(groups):
        g = lax.rem(me_ref[0] + groups - k, groups)
        product = dot(sums_refs[k][...], weight_ref[g], 0, 1)
        total = product if total is None else total + product
    out_ref[...] = total.astype(bf16)


def sum_parts_kernel(parts_ref, out_ref):
    total = parts_ref[0].astype(f32)
    for k in range(1, parts_ref.shape[0]):
        total = total + parts_ref[k].astype(f32)
    low = total.astype(bf16)
    for k in range(out_ref.shape[0]):
        out_ref[k] = low


def finish_kernel(parts_ref, key_ref, value_ref):
    for pair in range(parts_ref.shape[0] // 2):
        at = slice(pair * LANES, (pair + 1) * LANES)
        first = parts_ref[2 * pair].astype(f32).T
        second = parts_ref[2 * pair + 1].astype(f32).T
        key_ref[:, at], value_ref[:, at] = merge_pair(first, second)


def exchange(x, axes):
    return lax.all_to_all(x, axes, split_axis=0, concat_axis=0, tiled=True)


def shift(x, axis, size, by):
    return lax.ppermute(x, axis, [(k, (k + by) % size) for k in range(size)])


def per_device(inputs, w_key, w_value, queries, cotangent, cum_gate, **sizes):
    return program(inputs, w_key, w_value, queries, cotangent, cum_gate, **sizes)


def program(inputs, w_key, w_value, queries, cotangent, cum_gate, *, heads, dp, zs, xs):
    _, positions, features = inputs.shape
    kv_width = w_key.shape[1]
    rows = inputs.reshape(positions, features)
    me = lax.axis_index("x").astype(jnp.int32).reshape(1)
    to_head = [(head, head % zs * xs + head // zs) for head in range(heads)]

    packed = call(
        functools.partial(pack_queries_kernel, members=zs),
        shape((heads, positions, LANES)),
        queries.reshape(positions, -1), cotangent.reshape(positions, -1),
    )
    head_rows = exchange(packed, SP).reshape(heads * positions, LANES)
    cum = lax.ppermute(cum_gate[0], SP, to_head)
    near_rows = [rows] + [shift(rows, "x", xs, k) for k in range(1, xs)]
    weight = call(pack_weights_kernel, shape((w_key.shape[0], LANES)), me, w_key, w_value)
    weight = lax.all_gather(weight, "dp", axis=0, tiled=True)
    projected, copies = call(
        project_kernel,
        (shape((zs, xs, positions, LANES)), shape((xs, features, LANES))),
        me, weight, *near_rows,
    )
    head_kv = exchange(projected, "z").reshape(heads * positions, LANES)
    head_kv, copies = lax.optimization_barrier((head_kv, copies))
    weights = exchange(copies, "x")

    dq, dkv, grad_cum = attend(head_rows, head_kv, cum, xs)
    terms = exchange(dkv, "z")
    query_parts = exchange(dq, SP)
    *sums, part = call(
        group_sum_kernel,
        (*[shape((LANES, positions))] * xs, shape((dp, LANES, LANES))),
        me, terms, *near_rows,
    )
    own_sums = [sums[0]] + [shift(sums[k], "x", xs, k) for k in range(1, xs)]
    grad_input = call(grad_input_kernel, shape((positions, features)), me, weights, *own_sums)
    grad_cum = lax.ppermute(grad_cum, SP, [(b, a) for a, b in to_head])
    parts = exchange(part, "dp")
    grad_queries = call(
        functools.partial(unpack_queries_kernel, members=zs),
        shape((positions, features)), query_parts,
    )
    along = call(sum_parts_kernel, shape((zs, LANES, LANES)), parts)
    along = exchange(along, "z")
    along = call(sum_parts_kernel, shape((xs, LANES, LANES)), along)
    along = exchange(along, "x")
    half = shape((LANES, kv_width), f32)
    grad_key, grad_value = call(finish_kernel, (half, half), along)
    return grad_input[None], grad_queries[None], grad_cum[None], grad_key, grad_value


def solution(mesh):
    sizes = {"heads": mesh.shape["sp"], "dp": mesh.shape["dp"], "zs": 8, "xs": 4}
    split = Mesh(mesh.devices.reshape(sizes["zs"], sizes["xs"], sizes["dp"]), ("z", "x", "dp"))
    rows = P("dp", SP, None)
    weights = P("dp", None)
    return jax.shard_map(
        functools.partial(per_device, **sizes),
        mesh=split,
        in_specs=(rows, weights, weights, rows, rows, rows),
        out_specs=(rows, rows, rows, weights, weights),
        check_vma=False,
    )
```

```python
import functools

import jax
import jax.numpy as jnp
from jax import lax
from jax.experimental import pallas as pl
from jax.experimental.pallas import tpu as pltpu
from jax.sharding import Mesh
from jax.sharding import PartitionSpec as P


HD = 64
LANES = 128
LOG2E = 1.4426950408889634
BLOCK = 512
ONES = HD + 16
SP = ("zg", "zp", "x")
GROUP = ("zp", "x")
LOWEST = -3.4028235e38
bf16 = jnp.bfloat16
f32 = jnp.float32
VMEM = pltpu.VMEM


def dot(a, b, ca, cb):
    return lax.dot_general(a, b, (((ca,), (cb,)), ((), ())), preferred_element_type=f32)


def low_half(rows):
    return lax.broadcasted_iota(jnp.int32, (rows, LANES), 1) < HD


def merge_pair(a, b):
    low = low_half(a.shape[0])
    return jnp.where(low, a, pltpu.roll(b, HD, 1)), jnp.where(low, pltpu.roll(a, HD, 1), b)


def pieces(value):
    first = value.astype(bf16).astype(f32)
    rest = value - first
    second = rest.astype(bf16).astype(f32)
    third = (rest - second).astype(bf16).astype(f32)
    return first, second, third


def call(kernel, out_shapes, *args, scratch=(), vmem=60):
    many = isinstance(out_shapes, tuple)
    specs = pl.BlockSpec(memory_space=VMEM)
    return pl.pallas_call(
        kernel,
        out_shape=out_shapes,
        in_specs=[
            pl.BlockSpec(memory_space=pltpu.SMEM) if arg.dtype == jnp.int32 else specs
            for arg in args
        ],
        out_specs=(specs,) * len(out_shapes) if many else specs,
        scratch_shapes=scratch,
        compiler_params=pltpu.CompilerParams(vmem_limit_bytes=vmem * 1024 * 1024),
    )(*args)


def shape(dims, dtype=bf16):
    return jax.ShapeDtypeStruct(dims, dtype)


def pack_weights_kernel(key_ref, value_ref, out_ref):
    for pair in range(key_ref.shape[1] // LANES):
        at = slice(pair * LANES, (pair + 1) * LANES)
        blocks = merge_pair(key_ref[:, at].astype(f32), value_ref[:, at].astype(f32))
        for k in range(2):
            g = 2 * pair + k
            out_ref[:, g * LANES : (g + 1) * LANES] = blocks[k].astype(bf16)


def pack_queries_kernel(query_ref, grad_ref, out_ref):
    for pair in range(out_ref.shape[0] // 2):
        at = slice(pair * LANES, (pair + 1) * LANES)
        blocks = merge_pair(query_ref[:, at].astype(f32), grad_ref[:, at].astype(f32))
        for k in range(2):
            out_ref[2 * pair + k] = blocks[k].astype(bf16)


def project_kernel(rows_ref, weight_ref, out_ref):
    projected = dot(rows_ref[...], weight_ref[...], 1, 0).astype(bf16)
    for g in range(out_ref.shape[0]):
        out_ref[g] = projected[:, g * LANES : (g + 1) * LANES]


def copies_kernel(x_ref, out_ref):
    for k in range(out_ref.shape[0]):
        out_ref[k] = x_ref[...]


def attend_kernel(
    x_ref, parts_ref, cum_ref, dq_ref, dkv_ref, gcum_ref,
    kv_ref, qa_ref, ka_ref, kn_ref, s_ref, dp_ref, xt_ref, dkt_ref, dvt_ref, rows_ref, acc_ref, stat_ref,
    *, blk, seq,
):
    count = seq // blk
    members = dkv_ref.shape[0]
    scale = HD**-0.5
    lane = lax.broadcasted_iota(jnp.int32, (blk, LANES), 1)
    low = lane < HD
    row_id = lax.broadcasted_iota(jnp.int32, (LANES, blk), 0)

    def span(i):
        return pl.ds(pl.multiple_of(i * blk, blk), blk)

    def prepare(i, _):
        at = span(i)
        x = x_ref[at, :].astype(f32)
        for b in range(blk // LANES):
            owner = i * (blk // LANES) + b
            block = parts_ref[lax.rem(owner, members), lax.div(owner, members)]
            kv_ref[pl.ds(pl.multiple_of(owner * LANES, LANES), LANES), :] = block
        kv = kv_ref[at, :].astype(f32)
        c1, c2, c3 = pieces(jnp.broadcast_to(cum_ref[:, at] * LOG2E, (LANES, blk)))
        one = jnp.ones_like(c1)

        def extra(values):
            total = jnp.zeros_like(c1)
            for k, value in enumerate(values):
                total = jnp.where(row_id == HD + k, value, total)
            return total.T

        q1, q2, q3 = pieces(x * (LOG2E * scale))
        qa_ref[at, 0:LANES] = jnp.where(low, q1, pltpu.roll(q2, HD, 1)).astype(bf16)
        qa_ref[at, LANES:] = jnp.where(low, q3, extra((c1, c2, c3, one, one, one))).astype(bf16)
        ka_ref[at, 0:LANES] = jnp.where(low, kv, pltpu.roll(kv, HD, 1)).astype(bf16)
        ka_ref[at, LANES:] = jnp.where(low, kv, extra((one, one, one, -c1, -c2, -c3))).astype(bf16)
        kn_ref[at, :] = jnp.where(low, kv, jnp.where(lane == HD, 1.0, 0.0)).astype(bf16)
        xt = x.T
        ones_row = jnp.where(row_id == HD, 1.0, 0.0)
        xt_ref[0:ONES, at] = jnp.where(row_id < HD, xt, ones_row)[0:ONES].astype(bf16)
        xt_ref[ONES:, at] = xt[HD:].astype(bf16)
        dkt_ref[:, at] = jnp.zeros((ONES, blk), f32)
        dvt_ref[:, at] = jnp.zeros((HD, blk), f32)
        return 0

    lax.fori_loop(0, count, prepare, 0)

    def tiles(block):
        return [block[:, k * LANES : (k + 1) * LANES] for k in range(blk // LANES)]

    def query_block(i, _):
        rows = span(i)

        def score(j, diagonal):
            at = span(j)
            x = x_ref[rows, :]
            scores = dot(qa_ref[rows, :], ka_ref[at, :], 1, 1)
            if diagonal:
                sub = lax.broadcasted_iota(jnp.int32, (blk, blk), 0)
                col = lax.broadcasted_iota(jnp.int32, (blk, blk), 1)
                scores = jnp.where(col <= sub, scores, LOWEST)
            weights = dot(jnp.where(low, jnp.zeros_like(x), x), kv_ref[at, :], 1, 1)
            s_ref[:, at] = scores
            dp_ref[:, at] = weights
            return tiles(scores), tiles(weights)

        def tally(scores, weights, best):
            total = weighted = None
            for s, w in zip(scores, weights):
                e = jnp.exp2(s - best)
                total = e if total is None else total + e
                weighted = e * w if weighted is None else weighted + e * w
            return total, weighted

        scores, weights = score(i, True)
        best = functools.reduce(jnp.maximum, scores)
        stat_ref[0] = best
        stat_ref[1], stat_ref[2] = tally(scores, weights, best)

        def full_block(j, _):
            scores, weights = score(j, False)
            old = stat_ref[0]
            best = functools.reduce(jnp.maximum, scores, old)
            shrink = jnp.exp2(old - best)
            total, weighted = tally(scores, weights, best)
            stat_ref[0] = best
            stat_ref[1] = stat_ref[1] * shrink + total
            stat_ref[2] = stat_ref[2] * shrink + weighted
            return 0

        lax.fori_loop(0, i, full_block, 0)
        best = stat_ref[0]
        top = jnp.max(best, axis=1, keepdims=True)
        shrink = jnp.exp2(best - top)
        total = jnp.sum(stat_ref[1] * shrink, axis=1, keepdims=True)
        row_dot = jnp.sum(stat_ref[2] * shrink, axis=1, keepdims=True) / total
        stat_ref[0] = jnp.broadcast_to(top + jnp.log2(total), (blk, LANES))
        stat_ref[1] = jnp.broadcast_to(row_dot, (blk, LANES))
        acc_ref[...] = jnp.zeros((blk, LANES), f32)

        def gradients(j, _):
            at = span(j)
            level, row_dot = stat_ref[0], stat_ref[1]
            probs = [jnp.exp2(s - level) for s in tiles(s_ref[:, at])]
            grads = [p * (w - row_dot) for p, w in zip(probs, tiles(dp_ref[:, at]))]
            grad_low = jnp.concatenate([g.astype(bf16) for g in grads], axis=1)
            probs_low = jnp.concatenate([p.astype(bf16) for p in probs], axis=1)
            acc_ref[...] += dot(grad_low, kn_ref[at, :], 1, 0)
            dkt_ref[:, at] += dot(xt_ref[0:ONES, rows], grad_low, 1, 0)
            dvt_ref[:, at] += dot(xt_ref[ONES:, rows], probs_low, 1, 0)
            return 0

        lax.fori_loop(0, i + 1, gradients, 0)
        dq = acc_ref[...]
        rows_ref[:, rows] = dq.T[HD : HD + 8]
        dq = dq * scale
        for b in range(blk // LANES):
            upper = dq[b * LANES : b * LANES + HD]
            lower = dq[b * LANES + HD : (b + 1) * LANES]
            packed = jnp.where(low[0:HD], upper, pltpu.roll(lower, HD, 1))
            dq_ref[i * (blk // LANES) + b] = packed.astype(bf16)
        return 0

    lax.fori_loop(0, count, query_block, 0)
    for b in range(seq // LANES):
        at = slice(b * LANES, (b + 1) * LANES)
        dkv_ref[b % members, b // members, 0:HD, :] = (dkt_ref[0:HD, at] * scale).astype(bf16)
        dkv_ref[b % members, b // members, HD:, :] = dvt_ref[:, at].astype(bf16)
    gcum_ref[...] = rows_ref[0:1, :] - dkt_ref[HD : HD + 1, :]


def attend(x, parts, cum):
    members = parts.shape[0]
    seq = x.shape[0]
    owners = seq // LANES
    return call(
        functools.partial(attend_kernel, blk=BLOCK, seq=seq),
        (
            shape((owners, HD, LANES)),
            shape((members, owners // members, LANES, LANES)),
            shape((1, seq), f32),
        ),
        x, parts, cum,
        scratch=[
            VMEM((seq, LANES), bf16),
            VMEM((seq, 2 * LANES), bf16),
            VMEM((seq, 2 * LANES), bf16),
            VMEM((seq, LANES), bf16),
            VMEM((BLOCK, seq), f32),
            VMEM((BLOCK, seq), f32),
            VMEM((ONES + HD, seq), bf16),
            VMEM((ONES, seq), f32),
            VMEM((HD, seq), f32),
            VMEM((8, seq), f32),
            VMEM((BLOCK, LANES), f32),
            VMEM((3, BLOCK, LANES), f32),
        ],
    )


def group_sum_kernel(me_ref, terms_ref, rows_ref, *refs):
    owners = terms_ref.shape[1]
    sums_refs, part_ref = refs[:owners], refs[owners]
    part = None
    for k in range(owners):
        owner = lax.rem(me_ref[0] + k, owners)
        total = terms_ref[0, owner].astype(f32)
        for member in range(1, terms_ref.shape[0]):
            total = total + terms_ref[member, owner].astype(f32)
        low = total.astype(bf16)
        sums_refs[k][...] = low
        product = dot(low, rows_ref[owner], 1, 0)
        part = product if part is None else part + product
    for chunk in range(part_ref.shape[0]):
        part_ref[chunk] = part[:, chunk * LANES : (chunk + 1) * LANES].astype(bf16)


def unpack_queries_kernel(packed_ref, out_ref):
    for pair in range(packed_ref.shape[0] // 2):
        upper, lower = merge_pair(
            packed_ref[2 * pair].astype(f32), packed_ref[2 * pair + 1].astype(f32)
        )
        at = slice(pair * LANES, (pair + 1) * LANES)
        out_ref[0:HD, at] = upper.astype(bf16)
        out_ref[HD:, at] = lower.astype(bf16)


def grad_input_kernel(me_ref, weight_ref, *refs):
    sums_refs, out_ref = refs[:-1], refs[-1]
    groups = len(sums_refs)
    total = None
    for k in range(groups):
        g = lax.rem(me_ref[0] + groups - k, groups)
        columns = pl.ds(pl.multiple_of(g * LANES, LANES), LANES)
        product = dot(sums_refs[k][...], weight_ref[:, columns], 0, 1)
        total = product if total is None else total + product
    out_ref[...] = total.astype(bf16)


def sum_parts_kernel(parts_ref, out_ref):
    total = parts_ref[0].astype(f32)
    for k in range(1, parts_ref.shape[0]):
        total = total + parts_ref[k].astype(f32)
    low = total.astype(bf16)
    for k in range(out_ref.shape[0]):
        out_ref[k] = low


def finish_kernel(parts_ref, key_ref, value_ref):
    for pair in range(parts_ref.shape[0] // 2):
        at = slice(pair * LANES, (pair + 1) * LANES)
        first = parts_ref[2 * pair].astype(f32).T
        second = parts_ref[2 * pair + 1].astype(f32).T
        key_ref[:, at], value_ref[:, at] = merge_pair(first, second)


def exchange(x, axes):
    return lax.all_to_all(x, axes, split_axis=0, concat_axis=0, tiled=True)


def gather(x, axes, tiled):
    return lax.all_gather(x, axes, axis=0, tiled=tiled)


def shift(x, axis, size, by):
    return lax.ppermute(x, axis, [(k, (k + by) % size) for k in range(size)])


def per_device(inputs, w_key, w_value, queries, cotangent, cum_gate, **sizes):
    return program(inputs, w_key, w_value, queries, cotangent, cum_gate, **sizes)


def program(inputs, w_key, w_value, queries, cotangent, cum_gate, *, heads, dp, zg, zp, xs):
    _, positions, features = inputs.shape
    kv_width = w_key.shape[1]
    kv_heads = kv_width // HD
    members = zp * xs
    rows = inputs.reshape(positions, features)
    me = lax.axis_index("zg").astype(jnp.int32).reshape(1)

    weight = call(pack_weights_kernel, shape((w_key.shape[0], 2 * kv_width)), w_key, w_value)
    weight = gather(weight, "dp", True)
    packed = call(
        pack_queries_kernel, shape((heads, positions, LANES)),
        queries.reshape(positions, -1), cotangent.reshape(positions, -1),
    )
    head_rows = exchange(packed, SP).reshape(heads * positions, LANES)
    projected = call(project_kernel, shape((kv_heads, positions, LANES)), rows, weight)
    group_kv = exchange(projected, "zg")
    copies = call(copies_kernel, shape((members, *group_kv.shape)), group_kv)
    head_kv = exchange(copies, GROUP)
    head_kv, late_rows = lax.optimization_barrier((head_kv, rows))
    near_rows = gather(late_rows, "zg", False)

    dq, dkv, grad_cum = attend(head_rows, head_kv, cum_gate[0])
    terms = exchange(dkv, GROUP)
    query_parts = exchange(dq, SP)
    *sums, part = call(
        group_sum_kernel,
        (*[shape((LANES, positions))] * zg, shape((dp, LANES, LANES))),
        me, terms, near_rows,
    )
    own_sums = [sums[0]] + [shift(sums[k], "zg", zg, k) for k in range(1, zg)]
    grad_input = call(grad_input_kernel, shape((positions, features)), me, weight, *own_sums)
    parts = exchange(part, "dp")
    grad_queries = call(unpack_queries_kernel, shape((positions, features)), query_parts)
    along = call(sum_parts_kernel, shape((members, LANES, LANES)), parts)
    along = exchange(along, GROUP)
    along = call(sum_parts_kernel, shape((zg, LANES, LANES)), along)
    along = exchange(along, "zg")
    half = shape((LANES, kv_width), f32)
    grad_key, grad_value = call(finish_kernel, (half, half), along)
    return grad_input[None], grad_queries[None], grad_cum[None], grad_key, grad_value


def solution(mesh):
    sizes = {"heads": mesh.shape["sp"], "dp": mesh.shape["dp"], "zg": 4, "zp": 2, "xs": 4}
    split = Mesh(
        mesh.devices.reshape(sizes["zg"], sizes["zp"], sizes["xs"], sizes["dp"]),
        ("zg", "zp", "x", "dp"),
    )
    rows = P("dp", SP, None)
    weights = P("dp", None)
    return jax.shard_map(
        functools.partial(per_device, **sizes),
        mesh=split,
        in_specs=(rows, weights, weights, rows, rows, rows),
        out_specs=(rows, rows, rows, weights, weights),
        check_vma=False,
    )
```

```python
import functools

import jax
import jax.numpy as jnp
from jax import lax
from jax.experimental import pallas as pl
from jax.experimental.pallas import tpu as pltpu
from jax.sharding import Mesh
from jax.sharding import PartitionSpec as P


HD = 64
LANES = 128
LOG2E = 1.4426950408889634
BLOCK = 1024
STRIP = 32
PARTS = 4
GRAD_PARTS = 1
ONES = HD + 16
SP = ("zg", "zp", "x")
GROUP = ("zp", "x")
LOWEST = -3.4028235e38
bf16 = jnp.bfloat16
f32 = jnp.float32
VMEM = pltpu.VMEM


def dot(a, b, ca, cb):
    return lax.dot_general(a, b, (((ca,), (cb,)), ((), ())), preferred_element_type=f32)


def low_half(rows):
    return lax.broadcasted_iota(jnp.int32, (rows, LANES), 1) < HD


def merge_pair(a, b):
    low = low_half(a.shape[0])
    return jnp.where(low, a, pltpu.roll(b, HD, 1)), jnp.where(low, pltpu.roll(a, HD, 1), b)


def pieces(value):
    first = value.astype(bf16).astype(f32)
    rest = value - first
    second = rest.astype(bf16).astype(f32)
    third = (rest - second).astype(bf16).astype(f32)
    return first, second, third


def call(kernel, out_shapes, *args, scratch=(), vmem=60):
    many = isinstance(out_shapes, tuple)
    specs = pl.BlockSpec(memory_space=VMEM)
    return pl.pallas_call(
        kernel,
        out_shape=out_shapes,
        in_specs=[
            pl.BlockSpec(memory_space=pltpu.SMEM) if arg.dtype == jnp.int32 else specs
            for arg in args
        ],
        out_specs=(specs,) * len(out_shapes) if many else specs,
        scratch_shapes=scratch,
        compiler_params=pltpu.CompilerParams(vmem_limit_bytes=vmem * 1024 * 1024),
    )(*args)


def shape(dims, dtype=bf16):
    return jax.ShapeDtypeStruct(dims, dtype)


def pack_weights_kernel(key_ref, value_ref, out_ref):
    for pair in range(key_ref.shape[1] // LANES):
        at = slice(pair * LANES, (pair + 1) * LANES)
        blocks = merge_pair(key_ref[:, at].astype(f32), value_ref[:, at].astype(f32))
        for k in range(2):
            g = 2 * pair + k
            out_ref[:, g * LANES : (g + 1) * LANES] = blocks[k].astype(bf16)


def pack_queries_kernel(query_ref, grad_ref, out_ref):
    for pair in range(out_ref.shape[0] // 2):
        at = slice(pair * LANES, (pair + 1) * LANES)
        blocks = merge_pair(query_ref[:, at].astype(f32), grad_ref[:, at].astype(f32))
        for k in range(2):
            out_ref[2 * pair + k] = blocks[k].astype(bf16)


def project_kernel(rows_ref, weight_ref, out_ref):
    projected = dot(rows_ref[...], weight_ref[...], 1, 0).astype(bf16)
    for g in range(out_ref.shape[0]):
        out_ref[g] = projected[:, g * LANES : (g + 1) * LANES]


def copies_kernel(x_ref, out_ref):
    for k in range(out_ref.shape[0]):
        out_ref[k] = x_ref[...]


def attend_kernel(
    x_ref, parts_ref, cum_ref, dq_ref, dkv_ref, gcum_ref,
    kv_ref, qa_ref, ka_ref, kn_ref, s_ref, dp_ref, xt_ref, dkt_ref, dvt_ref, rows_ref, acc_ref, stat_ref,
    *, blk, seq,
):
    count = seq // blk
    members = dkv_ref.shape[0]
    scale = HD**-0.5
    lane = lax.broadcasted_iota(jnp.int32, (blk, LANES), 1)
    low = lane < HD
    row_id = lax.broadcasted_iota(jnp.int32, (LANES, blk), 0)

    def span(i):
        return pl.ds(pl.multiple_of(i * blk, blk), blk)

    def prepare(i, _):
        at = span(i)
        x = x_ref[at, :].astype(f32)
        for b in range(blk // LANES):
            owner = i * (blk // LANES) + b
            block = parts_ref[lax.rem(owner, members), lax.div(owner, members)]
            kv_ref[pl.ds(pl.multiple_of(owner * LANES, LANES), LANES), :] = block
        kv = kv_ref[at, :].astype(f32)
        c1, c2, c3 = pieces(jnp.broadcast_to(cum_ref[:, at] * LOG2E, (LANES, blk)))
        one = jnp.ones_like(c1)

        def extra(values):
            total = jnp.zeros_like(c1)
            for k, value in enumerate(values):
                total = jnp.where(row_id == HD + k, value, total)
            return total.T

        q1, q2, q3 = pieces(x * (LOG2E * scale))
        qa_ref[at, 0:LANES] = jnp.where(low, q1, pltpu.roll(q2, HD, 1)).astype(bf16)
        qa_ref[at, LANES:] = jnp.where(low, q3, extra((c1, c2, c3, one, one, one))).astype(bf16)
        ka_ref[at, 0:LANES] = jnp.where(low, kv, pltpu.roll(kv, HD, 1)).astype(bf16)
        ka_ref[at, LANES:] = jnp.where(low, kv, extra((one, one, one, -c1, -c2, -c3))).astype(bf16)
        kn_ref[at, :] = jnp.where(low, kv, jnp.where(lane == HD, 1.0, 0.0)).astype(bf16)
        xt = x.T
        ones_row = jnp.where(row_id == HD, 1.0, 0.0)
        xt_ref[0:ONES, at] = jnp.where(row_id < HD, xt, ones_row)[0:ONES].astype(bf16)
        xt_ref[ONES:, at] = xt[HD:].astype(bf16)
        dkt_ref[:, at] = jnp.zeros((ONES, blk), f32)
        dvt_ref[:, at] = jnp.zeros((HD, blk), f32)
        return 0

    lax.fori_loop(0, count, prepare, 0)

    def tiles(block):
        return [block[:, k * LANES : (k + 1) * LANES] for k in range(block.shape[1] // LANES)]

    half = blk // 2

    def query_block(i, _):
        def columns(j, width):
            return pl.ds(pl.multiple_of(j * blk, blk), width)

        def own_rows(first, size):
            return pl.ds(pl.multiple_of(i * blk + first, size), size)

        def score(first, size, at, width, diagonal):
            own = own_rows(first, size)
            x = x_ref[own, :]
            here = slice(first, first + size)
            scores = dot(qa_ref[own, :], ka_ref[at, :], 1, 1)
            if diagonal:
                sub = lax.broadcasted_iota(jnp.int32, (size, width), 0) + first
                col = lax.broadcasted_iota(jnp.int32, (size, width), 1)
                scores = jnp.where(col <= sub, scores, LOWEST)
            s_ref[here, at] = scores
            dp_ref[here, at] = dot(jnp.where(low_half(size), jnp.zeros_like(x), x), kv_ref[at, :], 1, 1)
            for strip in range(size // STRIP):
                part = slice(first + strip * STRIP, first + (strip + 1) * STRIP)
                scores, weights = tiles(s_ref[part, at]), tiles(dp_ref[part, at])
                if diagonal:
                    best = functools.reduce(jnp.maximum, scores)
                    total = weighted = jnp.zeros((STRIP, LANES), f32)
                else:
                    old = stat_ref[0, part]
                    best = functools.reduce(jnp.maximum, scores, old)
                    shrink = jnp.exp2(old - best)
                    total, weighted = stat_ref[1, part] * shrink, stat_ref[2, part] * shrink
                for s, w in zip(scores, weights):
                    e = jnp.exp2(s - best)
                    total, weighted = total + e, weighted + e * w
                stat_ref[0, part] = best
                stat_ref[1, part] = total
                stat_ref[2, part] = weighted

        score(0, half, columns(i, half), half, True)
        score(half, half, columns(i, blk), blk, True)

        def full_block(j, _):
            for k in range(PARTS):
                score(k * blk // PARTS, blk // PARTS, columns(j, blk), blk, False)
            return 0

        lax.fori_loop(0, i, full_block, 0)
        best = stat_ref[0]
        top = jnp.max(best, axis=1, keepdims=True)
        shrink = jnp.exp2(best - top)
        total = jnp.sum(stat_ref[1] * shrink, axis=1, keepdims=True)
        row_dot = jnp.sum(stat_ref[2] * shrink, axis=1, keepdims=True) / total
        stat_ref[0] = jnp.broadcast_to(top + jnp.log2(total), (blk, LANES))
        stat_ref[1] = jnp.broadcast_to(row_dot, (blk, LANES))
        acc_ref[...] = jnp.zeros((blk, LANES), f32)

        def gradients(first, size, at):
            own = own_rows(first, size)
            here = slice(first, first + size)
            level, row_dot = stat_ref[0, here], stat_ref[1, here]
            probs = [jnp.exp2(s - level) for s in tiles(s_ref[here, at])]
            grads = [p * (w - row_dot) for p, w in zip(probs, tiles(dp_ref[here, at]))]
            grad_low = jnp.concatenate([g.astype(bf16) for g in grads], axis=1)
            probs_low = jnp.concatenate([p.astype(bf16) for p in probs], axis=1)
            acc_ref[here] += dot(grad_low, kn_ref[at, :], 1, 0)
            dkt_ref[:, at] += dot(xt_ref[0:ONES, own], grad_low, 1, 0)
            dvt_ref[:, at] += dot(xt_ref[ONES:, own], probs_low, 1, 0)

        def full_gradients(j, _):
            for k in range(GRAD_PARTS):
                gradients(k * blk // GRAD_PARTS, blk // GRAD_PARTS, columns(j, blk))
            return 0

        lax.fori_loop(0, i, full_gradients, 0)
        gradients(0, half, columns(i, half))
        gradients(half, half, columns(i, blk))
        rows = own_rows(0, blk)
        dq = acc_ref[...]
        rows_ref[:, rows] = dq.T[HD : HD + 8]
        dq = dq * scale
        for b in range(blk // LANES):
            upper = dq[b * LANES : b * LANES + HD]
            lower = dq[b * LANES + HD : (b + 1) * LANES]
            packed = jnp.where(low[0:HD], upper, pltpu.roll(lower, HD, 1))
            dq_ref[i * (blk // LANES) + b] = packed.astype(bf16)
        return 0

    lax.fori_loop(0, count, query_block, 0)
    for b in range(seq // LANES):
        at = slice(b * LANES, (b + 1) * LANES)
        dkv_ref[b % members, b // members, 0:HD, :] = (dkt_ref[0:HD, at] * scale).astype(bf16)
        dkv_ref[b % members, b // members, HD:, :] = dvt_ref[:, at].astype(bf16)
    gcum_ref[...] = rows_ref[0:1, :] - dkt_ref[HD : HD + 1, :]


def attend(x, parts, cum):
    members = parts.shape[0]
    seq = x.shape[0]
    owners = seq // LANES
    return call(
        functools.partial(attend_kernel, blk=BLOCK, seq=seq),
        (
            shape((owners, HD, LANES)),
            shape((members, owners // members, LANES, LANES)),
            shape((1, seq), f32),
        ),
        x, parts, cum,
        scratch=[
            VMEM((seq, LANES), bf16),
            VMEM((seq, 2 * LANES), bf16),
            VMEM((seq, 2 * LANES), bf16),
            VMEM((seq, LANES), bf16),
            VMEM((BLOCK, seq), f32),
            VMEM((BLOCK, seq), f32),
            VMEM((ONES + HD, seq), bf16),
            VMEM((ONES, seq), f32),
            VMEM((HD, seq), f32),
            VMEM((8, seq), f32),
            VMEM((BLOCK, LANES), f32),
            VMEM((3, BLOCK, LANES), f32),
        ],
    )


def group_sum_kernel(me_ref, terms_ref, rows_ref, *refs):
    owners = terms_ref.shape[1]
    sums_refs, part_ref = refs[:owners], refs[owners]
    part = None
    for k in range(owners):
        owner = lax.rem(me_ref[0] + k, owners)
        total = terms_ref[0, owner].astype(f32)
        for member in range(1, terms_ref.shape[0]):
            total = total + terms_ref[member, owner].astype(f32)
        low = total.astype(bf16)
        sums_refs[k][...] = low
        product = dot(low, rows_ref[owner], 1, 0)
        part = product if part is None else part + product
    for chunk in range(part_ref.shape[0]):
        part_ref[chunk] = part[:, chunk * LANES : (chunk + 1) * LANES].astype(bf16)


def unpack_queries_kernel(packed_ref, out_ref):
    for pair in range(packed_ref.shape[0] // 2):
        upper, lower = merge_pair(
            packed_ref[2 * pair].astype(f32), packed_ref[2 * pair + 1].astype(f32)
        )
        at = slice(pair * LANES, (pair + 1) * LANES)
        out_ref[0:HD, at] = upper.astype(bf16)
        out_ref[HD:, at] = lower.astype(bf16)


def grad_input_kernel(me_ref, weight_ref, *refs):
    sums_refs, out_ref = refs[:-1], refs[-1]
    groups = len(sums_refs)
    total = None
    for k in range(groups):
        g = lax.rem(me_ref[0] + groups - k, groups)
        columns = pl.ds(pl.multiple_of(g * LANES, LANES), LANES)
        product = dot(sums_refs[k][...], weight_ref[:, columns], 0, 1)
        total = product if total is None else total + product
    out_ref[...] = total.astype(bf16)


def sum_parts_kernel(parts_ref, out_ref):
    total = parts_ref[0].astype(f32)
    for k in range(1, parts_ref.shape[0]):
        total = total + parts_ref[k].astype(f32)
    low = total.astype(bf16)
    for k in range(out_ref.shape[0]):
        out_ref[k] = low


def finish_kernel(parts_ref, key_ref, value_ref):
    for pair in range(parts_ref.shape[0] // 2):
        at = slice(pair * LANES, (pair + 1) * LANES)
        first = parts_ref[2 * pair].astype(f32).T
        second = parts_ref[2 * pair + 1].astype(f32).T
        key_ref[:, at], value_ref[:, at] = merge_pair(first, second)


def exchange(x, axes):
    return lax.all_to_all(x, axes, split_axis=0, concat_axis=0, tiled=True)


def gather(x, axes, tiled):
    return lax.all_gather(x, axes, axis=0, tiled=tiled)


def shift(x, axis, size, by):
    return lax.ppermute(x, axis, [(k, (k + by) % size) for k in range(size)])


def per_device(inputs, w_key, w_value, queries, cotangent, cum_gate, **sizes):
    return program(inputs, w_key, w_value, queries, cotangent, cum_gate, **sizes)


def program(inputs, w_key, w_value, queries, cotangent, cum_gate, *, heads, dp, zg, zp, xs):
    _, positions, features = inputs.shape
    kv_width = w_key.shape[1]
    kv_heads = kv_width // HD
    members = zp * xs
    rows = inputs.reshape(positions, features)
    me = lax.axis_index("zg").astype(jnp.int32).reshape(1)

    weight = call(pack_weights_kernel, shape((w_key.shape[0], 2 * kv_width)), w_key, w_value)
    weight = gather(weight, "dp", True)
    packed = call(
        pack_queries_kernel, shape((heads, positions, LANES)),
        queries.reshape(positions, -1), cotangent.reshape(positions, -1),
    )
    head_rows = exchange(packed, SP).reshape(heads * positions, LANES)
    projected = call(project_kernel, shape((kv_heads, positions, LANES)), rows, weight)
    group_kv = exchange(projected, "zg")
    copies = call(copies_kernel, shape((members, *group_kv.shape)), group_kv)
    head_kv = exchange(copies, GROUP)
    head_kv, late_rows = lax.optimization_barrier((head_kv, rows))
    near_rows = gather(late_rows, "zg", False)

    dq, dkv, grad_cum = attend(head_rows, head_kv, cum_gate[0])
    terms = exchange(dkv, GROUP)
    query_parts = exchange(dq, SP)
    *sums, part = call(
        group_sum_kernel,
        (*[shape((LANES, positions))] * zg, shape((dp, LANES, LANES))),
        me, terms, near_rows,
    )
    own_sums = [sums[0]] + [shift(sums[k], "zg", zg, k) for k in range(1, zg)]
    grad_input = call(grad_input_kernel, shape((positions, features)), me, weight, *own_sums)
    parts = exchange(part, "dp")
    grad_queries = call(unpack_queries_kernel, shape((positions, features)), query_parts)
    along = call(sum_parts_kernel, shape((members, LANES, LANES)), parts)
    along = exchange(along, GROUP)
    along = call(sum_parts_kernel, shape((zg, LANES, LANES)), along)
    along = exchange(along, "zg")
    half = shape((LANES, kv_width), f32)
    grad_key, grad_value = call(finish_kernel, (half, half), along)
    return grad_input[None], grad_queries[None], grad_cum[None], grad_key, grad_value


def solution(mesh):
    sizes = {"heads": mesh.shape["sp"], "dp": mesh.shape["dp"], "zg": 4, "zp": 2, "xs": 4}
    split = Mesh(
        mesh.devices.reshape(sizes["zg"], sizes["zp"], sizes["xs"], sizes["dp"]),
        ("zg", "zp", "x", "dp"),
    )
    rows = P("dp", SP, None)
    weights = P("dp", None)
    return jax.shard_map(
        functools.partial(per_device, **sizes),
        mesh=split,
        in_specs=(rows, weights, weights, rows, rows, rows),
        out_specs=(rows, rows, rows, weights, weights),
        check_vma=False,
    )
```

```python
import functools

import jax
import jax.numpy as jnp
from jax import lax
from jax.experimental import pallas as pl
from jax.experimental.pallas import tpu as pltpu
from jax.sharding import Mesh
from jax.sharding import PartitionSpec as P


HD = 64
LANES = 128
LOG2E = 1.4426950408889634
BLOCK = 1024
STRIP = 32
PARTS = 4
GRAD_PARTS = 1
ONES = HD + 16
SP = ("zg", "zp", "x")
GROUP = ("zp", "x")
LOWEST = -3.4028235e38
bf16 = jnp.bfloat16
f32 = jnp.float32
VMEM = pltpu.VMEM


def dot(a, b, ca, cb):
    return lax.dot_general(a, b, (((ca,), (cb,)), ((), ())), preferred_element_type=f32)


def low_half(rows):
    return lax.broadcasted_iota(jnp.int32, (rows, LANES), 1) < HD


def merge_pair(a, b):
    low = low_half(a.shape[0])
    return jnp.where(low, a, pltpu.roll(b, HD, 1)), jnp.where(low, pltpu.roll(a, HD, 1), b)


def pieces(value):
    first = value.astype(bf16).astype(f32)
    rest = value - first
    second = rest.astype(bf16).astype(f32)
    third = (rest - second).astype(bf16).astype(f32)
    return first, second, third


def call(kernel, out_shapes, *args, scratch=(), vmem=60):
    many = isinstance(out_shapes, tuple)
    specs = pl.BlockSpec(memory_space=VMEM)
    return pl.pallas_call(
        kernel,
        out_shape=out_shapes,
        in_specs=[
            pl.BlockSpec(memory_space=pltpu.SMEM) if arg.dtype == jnp.int32 else specs
            for arg in args
        ],
        out_specs=(specs,) * len(out_shapes) if many else specs,
        scratch_shapes=scratch,
        compiler_params=pltpu.CompilerParams(vmem_limit_bytes=vmem * 1024 * 1024),
    )(*args)


def shape(dims, dtype=bf16):
    return jax.ShapeDtypeStruct(dims, dtype)


def pack_weights_kernel(me_ref, key_ref, value_ref, all_ref, own_ref):
    for pair in range(key_ref.shape[1] // LANES):
        at = slice(pair * LANES, (pair + 1) * LANES)
        blocks = merge_pair(key_ref[:, at].astype(f32), value_ref[:, at].astype(f32))
        for k in range(2):
            g = 2 * pair + k
            all_ref[:, g * LANES : (g + 1) * LANES] = blocks[k].astype(bf16)
    own_ref[...] = all_ref[:, pl.ds(pl.multiple_of(me_ref[0] * LANES, LANES), LANES)]


def pack_queries_kernel(query_ref, grad_ref, out_ref):
    for pair in range(out_ref.shape[0] // 2):
        at = slice(pair * LANES, (pair + 1) * LANES)
        blocks = merge_pair(query_ref[:, at].astype(f32), grad_ref[:, at].astype(f32))
        for k in range(2):
            out_ref[2 * pair + k] = blocks[k].astype(bf16)


def project_kernel(rows_ref, weight_ref, out_ref):
    weight = weight_ref[...]
    for owner in range(rows_ref.shape[0]):
        projected = dot(rows_ref[owner], weight, 1, 0).astype(bf16)
        for member in range(out_ref.shape[0]):
            out_ref[member, owner] = projected


def attend_kernel(
    x_ref, parts_ref, cum_ref, dq_ref, dkv_ref, gcum_ref,
    kv_ref, qa_ref, ka_ref, kn_ref, s_ref, dp_ref, xt_ref, dkt_ref, dvt_ref, rows_ref, acc_ref, stat_ref,
    *, blk, seq,
):
    count = seq // blk
    members = dkv_ref.shape[0]
    scale = HD**-0.5
    lane = lax.broadcasted_iota(jnp.int32, (blk, LANES), 1)
    low = lane < HD
    row_id = lax.broadcasted_iota(jnp.int32, (LANES, blk), 0)

    def span(i):
        return pl.ds(pl.multiple_of(i * blk, blk), blk)

    def prepare(i, _):
        at = span(i)
        x = x_ref[at, :].astype(f32)
        for b in range(blk // LANES):
            owner = i * (blk // LANES) + b
            block = parts_ref[lax.rem(owner, members), lax.div(owner, members)]
            kv_ref[pl.ds(pl.multiple_of(owner * LANES, LANES), LANES), :] = block
        kv = kv_ref[at, :].astype(f32)
        c1, c2, c3 = pieces(jnp.broadcast_to(cum_ref[:, at] * LOG2E, (LANES, blk)))
        one = jnp.ones_like(c1)

        def extra(values):
            total = jnp.zeros_like(c1)
            for k, value in enumerate(values):
                total = jnp.where(row_id == HD + k, value, total)
            return total.T

        q1, q2, q3 = pieces(x * (LOG2E * scale))
        qa_ref[at, 0:LANES] = jnp.where(low, q1, pltpu.roll(q2, HD, 1)).astype(bf16)
        qa_ref[at, LANES:] = jnp.where(low, q3, extra((c1, c2, c3, one, one, one))).astype(bf16)
        ka_ref[at, 0:LANES] = jnp.where(low, kv, pltpu.roll(kv, HD, 1)).astype(bf16)
        ka_ref[at, LANES:] = jnp.where(low, kv, extra((one, one, one, -c1, -c2, -c3))).astype(bf16)
        kn_ref[at, :] = jnp.where(low, kv, jnp.where(lane == HD, 1.0, 0.0)).astype(bf16)
        xt = x.T
        ones_row = jnp.where(row_id == HD, 1.0, 0.0)
        xt_ref[0:ONES, at] = jnp.where(row_id < HD, xt, ones_row)[0:ONES].astype(bf16)
        xt_ref[ONES:, at] = xt[HD:].astype(bf16)
        dkt_ref[:, at] = jnp.zeros((ONES, blk), f32)
        dvt_ref[:, at] = jnp.zeros((HD, blk), f32)
        return 0

    lax.fori_loop(0, count, prepare, 0)

    def tiles(block):
        return [block[:, k * LANES : (k + 1) * LANES] for k in range(block.shape[1] // LANES)]

    half = blk // 2

    def query_block(i, _):
        def columns(j, width):
            return pl.ds(pl.multiple_of(j * blk, blk), width)

        def own_rows(first, size):
            return pl.ds(pl.multiple_of(i * blk + first, size), size)

        def score(first, size, at, width, diagonal):
            own = own_rows(first, size)
            x = x_ref[own, :]
            here = slice(first, first + size)
            scores = dot(qa_ref[own, :], ka_ref[at, :], 1, 1)
            if diagonal:
                sub = lax.broadcasted_iota(jnp.int32, (size, width), 0) + first
                col = lax.broadcasted_iota(jnp.int32, (size, width), 1)
                scores = jnp.where(col <= sub, scores, LOWEST)
            s_ref[here, at] = scores
            dp_ref[here, at] = dot(jnp.where(low_half(size), jnp.zeros_like(x), x), kv_ref[at, :], 1, 1)
            for strip in range(size // STRIP):
                part = slice(first + strip * STRIP, first + (strip + 1) * STRIP)
                scores, weights = tiles(s_ref[part, at]), tiles(dp_ref[part, at])
                if diagonal:
                    best = functools.reduce(jnp.maximum, scores)
                    total = weighted = jnp.zeros((STRIP, LANES), f32)
                else:
                    old = stat_ref[0, part]
                    best = functools.reduce(jnp.maximum, scores, old)
                    shrink = jnp.exp2(old - best)
                    total, weighted = stat_ref[1, part] * shrink, stat_ref[2, part] * shrink
                for s, w in zip(scores, weights):
                    e = jnp.exp2(s - best)
                    total, weighted = total + e, weighted + e * w
                stat_ref[0, part] = best
                stat_ref[1, part] = total
                stat_ref[2, part] = weighted

        score(0, half, columns(i, half), half, True)
        score(half, half, columns(i, blk), blk, True)

        def full_block(j, _):
            for k in range(PARTS):
                score(k * blk // PARTS, blk // PARTS, columns(j, blk), blk, False)
            return 0

        lax.fori_loop(0, i, full_block, 0)
        best = stat_ref[0]
        top = jnp.max(best, axis=1, keepdims=True)
        shrink = jnp.exp2(best - top)
        total = jnp.sum(stat_ref[1] * shrink, axis=1, keepdims=True)
        row_dot = jnp.sum(stat_ref[2] * shrink, axis=1, keepdims=True) / total
        stat_ref[0] = jnp.broadcast_to(top + jnp.log2(total), (blk, LANES))
        stat_ref[1] = jnp.broadcast_to(row_dot, (blk, LANES))
        acc_ref[...] = jnp.zeros((blk, LANES), f32)

        def gradients(first, size, at):
            own = own_rows(first, size)
            here = slice(first, first + size)
            level, row_dot = stat_ref[0, here], stat_ref[1, here]
            probs = [jnp.exp2(s - level) for s in tiles(s_ref[here, at])]
            grads = [p * (w - row_dot) for p, w in zip(probs, tiles(dp_ref[here, at]))]
            grad_low = jnp.concatenate([g.astype(bf16) for g in grads], axis=1)
            probs_low = jnp.concatenate([p.astype(bf16) for p in probs], axis=1)
            acc_ref[here] += dot(grad_low, kn_ref[at, :], 1, 0)
            dkt_ref[:, at] += dot(xt_ref[0:ONES, own], grad_low, 1, 0)
            dvt_ref[:, at] += dot(xt_ref[ONES:, own], probs_low, 1, 0)

        def full_gradients(j, _):
            for k in range(GRAD_PARTS):
                gradients(k * blk // GRAD_PARTS, blk // GRAD_PARTS, columns(j, blk))
            return 0

        lax.fori_loop(0, i, full_gradients, 0)
        gradients(0, half, columns(i, half))
        gradients(half, half, columns(i, blk))
        rows = own_rows(0, blk)
        dq = acc_ref[...]
        rows_ref[:, rows] = dq.T[HD : HD + 8]
        dq = dq * scale
        for b in range(blk // LANES):
            upper = dq[b * LANES : b * LANES + HD]
            lower = dq[b * LANES + HD : (b + 1) * LANES]
            packed = jnp.where(low[0:HD], upper, pltpu.roll(lower, HD, 1))
            dq_ref[i * (blk // LANES) + b] = packed.astype(bf16)
        return 0

    lax.fori_loop(0, count, query_block, 0)
    for b in range(seq // LANES):
        at = slice(b * LANES, (b + 1) * LANES)
        dkv_ref[b % members, b // members, 0:HD, :] = (dkt_ref[0:HD, at] * scale).astype(bf16)
        dkv_ref[b % members, b // members, HD:, :] = dvt_ref[:, at].astype(bf16)
    gcum_ref[...] = rows_ref[0:1, :] - dkt_ref[HD : HD + 1, :]


def attend(x, parts, cum):
    members = parts.shape[0]
    seq = x.shape[0]
    owners = seq // LANES
    return call(
        functools.partial(attend_kernel, blk=BLOCK, seq=seq),
        (
            shape((owners, HD, LANES)),
            shape((members, owners // members, LANES, LANES)),
            shape((1, seq), f32),
        ),
        x, parts, cum,
        scratch=[
            VMEM((seq, LANES), bf16),
            VMEM((seq, 2 * LANES), bf16),
            VMEM((seq, 2 * LANES), bf16),
            VMEM((seq, LANES), bf16),
            VMEM((BLOCK, seq), f32),
            VMEM((BLOCK, seq), f32),
            VMEM((ONES + HD, seq), bf16),
            VMEM((ONES, seq), f32),
            VMEM((HD, seq), f32),
            VMEM((8, seq), f32),
            VMEM((BLOCK, LANES), f32),
            VMEM((3, BLOCK, LANES), f32),
        ],
    )


def group_sum_kernel(me_ref, terms_ref, rows_ref, *refs):
    owners = terms_ref.shape[1]
    sums_refs, part_ref = refs[:owners], refs[owners]
    part = None
    for k in range(owners):
        owner = lax.rem(me_ref[0] + k, owners)
        total = terms_ref[0, owner].astype(f32)
        for member in range(1, terms_ref.shape[0]):
            total = total + terms_ref[member, owner].astype(f32)
        low = total.astype(bf16)
        sums_refs[k][...] = low
        product = dot(low, rows_ref[owner], 1, 0)
        part = product if part is None else part + product
    for chunk in range(part_ref.shape[0]):
        part_ref[chunk] = part[:, chunk * LANES : (chunk + 1) * LANES].astype(bf16)


def unpack_queries_kernel(packed_ref, out_ref):
    for pair in range(packed_ref.shape[0] // 2):
        upper, lower = merge_pair(
            packed_ref[2 * pair].astype(f32), packed_ref[2 * pair + 1].astype(f32)
        )
        at = slice(pair * LANES, (pair + 1) * LANES)
        out_ref[0:HD, at] = upper.astype(bf16)
        out_ref[HD:, at] = lower.astype(bf16)


def grad_input_kernel(me_ref, weight_ref, *refs):
    sums_refs, out_ref = refs[:-1], refs[-1]
    groups = len(sums_refs)
    total = None
    for k in range(groups):
        g = lax.rem(me_ref[0] + groups - k, groups)
        columns = pl.ds(pl.multiple_of(g * LANES, LANES), LANES)
        product = dot(sums_refs[k][...], weight_ref[:, columns], 0, 1)
        total = product if total is None else total + product
    out_ref[...] = total.astype(bf16)


def sum_parts_kernel(parts_ref, out_ref):
    total = parts_ref[0].astype(f32)
    for k in range(1, parts_ref.shape[0]):
        total = total + parts_ref[k].astype(f32)
    low = total.astype(bf16)
    for k in range(out_ref.shape[0]):
        out_ref[k] = low


def finish_kernel(parts_ref, key_ref, value_ref):
    for pair in range(parts_ref.shape[0] // 2):
        at = slice(pair * LANES, (pair + 1) * LANES)
        first = parts_ref[2 * pair].astype(f32).T
        second = parts_ref[2 * pair + 1].astype(f32).T
        key_ref[:, at], value_ref[:, at] = merge_pair(first, second)


def exchange(x, axes):
    return lax.all_to_all(x, axes, split_axis=0, concat_axis=0, tiled=True)


def gather(x, axes, tiled):
    return lax.all_gather(x, axes, axis=0, tiled=tiled)


def shift(x, axis, size, by):
    return lax.ppermute(x, axis, [(k, (k + by) % size) for k in range(size)])


def per_device(inputs, w_key, w_value, queries, cotangent, cum_gate, **sizes):
    return program(inputs, w_key, w_value, queries, cotangent, cum_gate, **sizes)


def program(inputs, w_key, w_value, queries, cotangent, cum_gate, *, heads, dp, zg, zp, xs):
    _, positions, features = inputs.shape
    kv_width = w_key.shape[1]
    members = zp * xs
    rows = inputs.reshape(positions, features)
    me = lax.axis_index("zg").astype(jnp.int32).reshape(1)

    near_rows = gather(rows, "zg", False)
    packed = call(
        pack_queries_kernel, shape((heads, positions, LANES)),
        queries.reshape(positions, -1), cotangent.reshape(positions, -1),
    )
    head_rows = exchange(packed, SP).reshape(heads * positions, LANES)
    depth = w_key.shape[0]
    local, own = call(
        pack_weights_kernel,
        (shape((depth, 2 * kv_width)), shape((depth, LANES))),
        me, w_key, w_value,
    )
    weights = gather(local, "dp", True)
    weight = gather(own, "dp", True)
    projected = call(project_kernel, shape((members, zg, positions, LANES)), near_rows, weight)
    head_kv = exchange(projected, GROUP)

    dq, dkv, grad_cum = attend(head_rows, head_kv, cum_gate[0])
    terms = exchange(dkv, GROUP)
    query_parts = exchange(dq, SP)
    *sums, part = call(
        group_sum_kernel,
        (*[shape((LANES, positions))] * zg, shape((dp, LANES, LANES))),
        me, terms, near_rows,
    )
    own_sums = [sums[0]] + [shift(sums[k], "zg", zg, k) for k in range(1, zg)]
    grad_input = call(grad_input_kernel, shape((positions, features)), me, weights, *own_sums)
    parts = exchange(part, "dp")
    grad_queries = call(unpack_queries_kernel, shape((positions, features)), query_parts)
    along = call(sum_parts_kernel, shape((members, LANES, LANES)), parts)
    along = exchange(along, GROUP)
    along = call(sum_parts_kernel, shape((zg, LANES, LANES)), along)
    along = exchange(along, "zg")
    half = shape((LANES, kv_width), f32)
    grad_key, grad_value = call(finish_kernel, (half, half), along)
    return grad_input[None], grad_queries[None], grad_cum[None], grad_key, grad_value


def solution(mesh):
    sizes = {"heads": mesh.shape["sp"], "dp": mesh.shape["dp"], "zg": 4, "zp": 2, "xs": 4}
    split = Mesh(
        mesh.devices.reshape(sizes["zg"], sizes["zp"], sizes["xs"], sizes["dp"]),
        ("zg", "zp", "x", "dp"),
    )
    rows = P("dp", SP, None)
    weights = P("dp", None)
    return jax.shard_map(
        functools.partial(per_device, **sizes),
        mesh=split,
        in_specs=(rows, weights, weights, rows, rows, rows),
        out_specs=(rows, rows, rows, weights, weights),
        check_vma=False,
    )
```

```python
import functools

import jax
import jax.numpy as jnp
from jax import lax
from jax.experimental import pallas as pl
from jax.experimental.pallas import tpu as pltpu
from jax.sharding import Mesh
from jax.sharding import PartitionSpec as P


HD = 64
LANES = 128
LOG2E = 1.4426950408889634
BLOCK = 1024
STRIP = 32
PARTS = 4
GRAD_PARTS = 1
ONES = HD + 16
SP = ("zg", "zp", "x")
GROUP = ("zp", "x")
LOWEST = -3.4028235e38
bf16 = jnp.bfloat16
f32 = jnp.float32
VMEM = pltpu.VMEM


def dot(a, b, ca, cb):
    return lax.dot_general(a, b, (((ca,), (cb,)), ((), ())), preferred_element_type=f32)


def low_half(rows):
    return lax.broadcasted_iota(jnp.int32, (rows, LANES), 1) < HD


def merge_pair(a, b):
    low = low_half(a.shape[0])
    return jnp.where(low, a, pltpu.roll(b, HD, 1)), jnp.where(low, pltpu.roll(a, HD, 1), b)


def pieces(value):
    first = value.astype(bf16).astype(f32)
    rest = value - first
    second = rest.astype(bf16).astype(f32)
    third = (rest - second).astype(bf16).astype(f32)
    return first, second, third


def call(kernel, out_shapes, *args, scratch=(), vmem=60):
    many = isinstance(out_shapes, tuple)
    specs = pl.BlockSpec(memory_space=VMEM)
    return pl.pallas_call(
        kernel,
        out_shape=out_shapes,
        in_specs=[
            pl.BlockSpec(memory_space=pltpu.SMEM) if arg.dtype == jnp.int32 else specs
            for arg in args
        ],
        out_specs=(specs,) * len(out_shapes) if many else specs,
        scratch_shapes=scratch,
        compiler_params=pltpu.CompilerParams(vmem_limit_bytes=vmem * 1024 * 1024),
    )(*args)


def shape(dims, dtype=bf16):
    return jax.ShapeDtypeStruct(dims, dtype)


def pack_weights_kernel(key_ref, value_ref, out_ref):
    for pair in range(key_ref.shape[1] // LANES):
        at = slice(pair * LANES, (pair + 1) * LANES)
        blocks = merge_pair(key_ref[:, at].astype(f32), value_ref[:, at].astype(f32))
        for k in range(2):
            g = 2 * pair + k
            out_ref[:, g * LANES : (g + 1) * LANES] = blocks[k].astype(bf16)


def pack_queries_kernel(query_ref, grad_ref, out_ref):
    for pair in range(out_ref.shape[0] // 2):
        at = slice(pair * LANES, (pair + 1) * LANES)
        blocks = merge_pair(query_ref[:, at].astype(f32), grad_ref[:, at].astype(f32))
        for k in range(2):
            out_ref[2 * pair + k] = blocks[k].astype(bf16)


def project_kernel(rows_ref, weight_ref, out_ref):
    projected = dot(rows_ref[...], weight_ref[...], 1, 0).astype(bf16)
    for g in range(out_ref.shape[0]):
        out_ref[g] = projected[:, g * LANES : (g + 1) * LANES]


def attend_kernel(
    x_ref, parts_ref, cum_ref, dq_ref, dkv_ref, gcum_ref,
    kv_ref, qa_ref, ka_ref, kn_ref, s_ref, dp_ref, xt_ref, dkt_ref, dvt_ref, rows_ref, acc_ref, stat_ref,
    *, blk, seq,
):
    count = seq // blk
    members = dkv_ref.shape[0]
    scale = HD**-0.5
    lane = lax.broadcasted_iota(jnp.int32, (blk, LANES), 1)
    low = lane < HD
    row_id = lax.broadcasted_iota(jnp.int32, (LANES, blk), 0)

    def span(i):
        return pl.ds(pl.multiple_of(i * blk, blk), blk)

    def prepare(i, _):
        at = span(i)
        x = x_ref[at, :].astype(f32)
        for b in range(blk // LANES):
            owner = i * (blk // LANES) + b
            block = parts_ref[lax.rem(owner, members), lax.div(owner, members)]
            kv_ref[pl.ds(pl.multiple_of(owner * LANES, LANES), LANES), :] = block
        kv = kv_ref[at, :].astype(f32)
        c1, c2, c3 = pieces(jnp.broadcast_to(cum_ref[:, at] * LOG2E, (LANES, blk)))
        one = jnp.ones_like(c1)

        def extra(values):
            total = jnp.zeros_like(c1)
            for k, value in enumerate(values):
                total = jnp.where(row_id == HD + k, value, total)
            return total.T

        q1, q2, q3 = pieces(x * (LOG2E * scale))
        qa_ref[at, 0:LANES] = jnp.where(low, q1, pltpu.roll(q2, HD, 1)).astype(bf16)
        qa_ref[at, LANES:] = jnp.where(low, q3, extra((c1, c2, c3, one, one, one))).astype(bf16)
        ka_ref[at, 0:LANES] = jnp.where(low, kv, pltpu.roll(kv, HD, 1)).astype(bf16)
        ka_ref[at, LANES:] = jnp.where(low, kv, extra((one, one, one, -c1, -c2, -c3))).astype(bf16)
        kn_ref[at, :] = jnp.where(low, kv, jnp.where(lane == HD, 1.0, 0.0)).astype(bf16)
        xt = x.T
        ones_row = jnp.where(row_id == HD, 1.0, 0.0)
        xt_ref[0:ONES, at] = jnp.where(row_id < HD, xt, ones_row)[0:ONES].astype(bf16)
        xt_ref[ONES:, at] = xt[HD:].astype(bf16)
        dkt_ref[:, at] = jnp.zeros((ONES, blk), f32)
        dvt_ref[:, at] = jnp.zeros((HD, blk), f32)
        return 0

    lax.fori_loop(0, count, prepare, 0)

    def tiles(block):
        return [block[:, k * LANES : (k + 1) * LANES] for k in range(block.shape[1] // LANES)]

    half = blk // 2

    def query_block(i, _):
        def columns(j, width):
            return pl.ds(pl.multiple_of(j * blk, blk), width)

        def own_rows(first, size):
            return pl.ds(pl.multiple_of(i * blk + first, size), size)

        def score(first, size, at, width, diagonal):
            own = own_rows(first, size)
            x = x_ref[own, :]
            here = slice(first, first + size)
            scores = dot(qa_ref[own, :], ka_ref[at, :], 1, 1)
            if diagonal:
                sub = lax.broadcasted_iota(jnp.int32, (size, width), 0) + first
                col = lax.broadcasted_iota(jnp.int32, (size, width), 1)
                scores = jnp.where(col <= sub, scores, LOWEST)
            s_ref[here, at] = scores
            dp_ref[here, at] = dot(jnp.where(low_half(size), jnp.zeros_like(x), x), kv_ref[at, :], 1, 1)
            for strip in range(size // STRIP):
                part = slice(first + strip * STRIP, first + (strip + 1) * STRIP)
                scores, weights = tiles(s_ref[part, at]), tiles(dp_ref[part, at])
                if diagonal:
                    best = functools.reduce(jnp.maximum, scores)
                    total = weighted = jnp.zeros((STRIP, LANES), f32)
                else:
                    old = stat_ref[0, part]
                    best = functools.reduce(jnp.maximum, scores, old)
                    shrink = jnp.exp2(old - best)
                    total, weighted = stat_ref[1, part] * shrink, stat_ref[2, part] * shrink
                for s, w in zip(scores, weights):
                    e = jnp.exp2(s - best)
                    total, weighted = total + e, weighted + e * w
                stat_ref[0, part] = best
                stat_ref[1, part] = total
                stat_ref[2, part] = weighted

        score(0, half, columns(i, half), half, True)
        score(half, half, columns(i, blk), blk, True)

        def full_block(j, _):
            for k in range(PARTS):
                score(k * blk // PARTS, blk // PARTS, columns(j, blk), blk, False)
            return 0

        lax.fori_loop(0, i, full_block, 0)
        best = stat_ref[0]
        top = jnp.max(best, axis=1, keepdims=True)
        shrink = jnp.exp2(best - top)
        total = jnp.sum(stat_ref[1] * shrink, axis=1, keepdims=True)
        row_dot = jnp.sum(stat_ref[2] * shrink, axis=1, keepdims=True) / total
        stat_ref[0] = jnp.broadcast_to(top + jnp.log2(total), (blk, LANES))
        stat_ref[1] = jnp.broadcast_to(row_dot, (blk, LANES))
        acc_ref[...] = jnp.zeros((blk, LANES), f32)

        def gradients(first, size, at):
            own = own_rows(first, size)
            here = slice(first, first + size)
            level, row_dot = stat_ref[0, here], stat_ref[1, here]
            probs = [jnp.exp2(s - level) for s in tiles(s_ref[here, at])]
            grads = [p * (w - row_dot) for p, w in zip(probs, tiles(dp_ref[here, at]))]
            grad_low = jnp.concatenate([g.astype(bf16) for g in grads], axis=1)
            probs_low = jnp.concatenate([p.astype(bf16) for p in probs], axis=1)
            acc_ref[here] += dot(grad_low, kn_ref[at, :], 1, 0)
            dkt_ref[:, at] += dot(xt_ref[0:ONES, own], grad_low, 1, 0)
            dvt_ref[:, at] += dot(xt_ref[ONES:, own], probs_low, 1, 0)

        def full_gradients(j, _):
            for k in range(GRAD_PARTS):
                gradients(k * blk // GRAD_PARTS, blk // GRAD_PARTS, columns(j, blk))
            return 0

        lax.fori_loop(0, i, full_gradients, 0)
        gradients(0, half, columns(i, half))
        gradients(half, half, columns(i, blk))
        rows = own_rows(0, blk)
        dq = acc_ref[...]
        rows_ref[:, rows] = dq.T[HD : HD + 8]
        dq = dq * scale
        for b in range(blk // LANES):
            upper = dq[b * LANES : b * LANES + HD]
            lower = dq[b * LANES + HD : (b + 1) * LANES]
            packed = jnp.where(low[0:HD], upper, pltpu.roll(lower, HD, 1))
            dq_ref[i * (blk // LANES) + b] = packed.astype(bf16)
        return 0

    lax.fori_loop(0, count, query_block, 0)
    for b in range(seq // LANES):
        at = slice(b * LANES, (b + 1) * LANES)
        dkv_ref[b % members, b // members, 0:HD, :] = (dkt_ref[0:HD, at] * scale).astype(bf16)
        dkv_ref[b % members, b // members, HD:, :] = dvt_ref[:, at].astype(bf16)
    gcum_ref[...] = rows_ref[0:1, :] - dkt_ref[HD : HD + 1, :]


def attend(x, parts, cum):
    members = parts.shape[0]
    seq = x.shape[0]
    owners = seq // LANES
    return call(
        functools.partial(attend_kernel, blk=BLOCK, seq=seq),
        (
            shape((owners, HD, LANES)),
            shape((members, owners // members, LANES, LANES)),
            shape((1, seq), f32),
        ),
        x, parts, cum,
        scratch=[
            VMEM((seq, LANES), bf16),
            VMEM((seq, 2 * LANES), bf16),
            VMEM((seq, 2 * LANES), bf16),
            VMEM((seq, LANES), bf16),
            VMEM((BLOCK, seq), f32),
            VMEM((BLOCK, seq), f32),
            VMEM((ONES + HD, seq), bf16),
            VMEM((ONES, seq), f32),
            VMEM((HD, seq), f32),
            VMEM((8, seq), f32),
            VMEM((BLOCK, LANES), f32),
            VMEM((3, BLOCK, LANES), f32),
        ],
    )


def group_sum_kernel(me_ref, terms_ref, left_ref, right_ref, *refs):
    owners = terms_ref.shape[1]
    sums_refs, part_ref = refs[:owners], refs[owners]
    parts = None
    for k in range(owners):
        owner = lax.rem(me_ref[0] + k, owners)
        total = terms_ref[0, owner].astype(f32)
        for member in range(1, terms_ref.shape[0]):
            total = total + terms_ref[member, owner].astype(f32)
        low = total.astype(bf16)
        sums_refs[k][...] = low
        products = [dot(low, rows_ref[owner], 1, 0) for rows_ref in (left_ref, right_ref)]
        parts = products if parts is None else [p + q for p, q in zip(parts, products)]
    half = part_ref.shape[0] // 2
    for chunk in range(part_ref.shape[0]):
        at = slice(chunk % half * LANES, (chunk % half + 1) * LANES)
        part_ref[chunk] = parts[chunk // half][:, at].astype(bf16)


def unpack_queries_kernel(packed_ref, out_ref):
    for pair in range(packed_ref.shape[0] // 2):
        upper, lower = merge_pair(
            packed_ref[2 * pair].astype(f32), packed_ref[2 * pair + 1].astype(f32)
        )
        at = slice(pair * LANES, (pair + 1) * LANES)
        out_ref[0:HD, at] = upper.astype(bf16)
        out_ref[HD:, at] = lower.astype(bf16)


def grad_input_kernel(me_ref, weight_ref, *refs):
    sums_refs, out_ref = refs[:-1], refs[-1]
    groups = len(sums_refs)
    total = None
    for k in range(groups):
        g = lax.rem(me_ref[0] + groups - k, groups)
        columns = pl.ds(pl.multiple_of(g * LANES, LANES), LANES)
        product = dot(sums_refs[k][...], weight_ref[:, columns], 0, 1)
        total = product if total is None else total + product
    out_ref[...] = total.astype(bf16)


def sum_parts_kernel(parts_ref, out_ref):
    total = parts_ref[0].astype(f32)
    for k in range(1, parts_ref.shape[0]):
        total = total + parts_ref[k].astype(f32)
    low = total.astype(bf16)
    for k in range(out_ref.shape[0]):
        out_ref[k] = low


def finish_kernel(parts_ref, key_ref, value_ref):
    for pair in range(parts_ref.shape[0] // 2):
        at = slice(pair * LANES, (pair + 1) * LANES)
        first = parts_ref[2 * pair].astype(f32).T
        second = parts_ref[2 * pair + 1].astype(f32).T
        key_ref[:, at], value_ref[:, at] = merge_pair(first, second)


def exchange(x, axes):
    return lax.all_to_all(x, axes, split_axis=0, concat_axis=0, tiled=True)


def gather(x, axes, tiled):
    return lax.all_gather(x, axes, axis=0, tiled=tiled)


def shift(x, axis, size, by):
    return lax.ppermute(x, axis, [(k, (k + by) % size) for k in range(size)])


def per_device(inputs, w_key, w_value, queries, cotangent, cum_gate, **sizes):
    return program(inputs, w_key, w_value, queries, cotangent, cum_gate, **sizes)


def program(inputs, w_key, w_value, queries, cotangent, cum_gate, *, heads, dp, zg, zp, xs):
    _, positions, features = inputs.shape
    kv_width = w_key.shape[1]
    kv_heads = kv_width // HD
    members = zp * xs
    rows = inputs.reshape(positions, features)
    me = lax.axis_index("zg").astype(jnp.int32).reshape(1)

    weight = call(pack_weights_kernel, shape((w_key.shape[0], 2 * kv_width)), w_key, w_value)
    weight = gather(weight, "dp", True)
    packed = call(
        pack_queries_kernel, shape((heads, positions, LANES)),
        queries.reshape(positions, -1), cotangent.reshape(positions, -1),
    )
    head_rows = exchange(packed, SP).reshape(heads * positions, LANES)
    projected = call(project_kernel, shape((kv_heads, positions, LANES)), rows, weight)
    group_kv = exchange(projected, "zg")
    copies = jnp.broadcast_to(group_kv[None], (members, *group_kv.shape))
    head_kv = exchange(copies, GROUP)
    half = features // 2
    near_rows = [gather(rows[:, k * half : (k + 1) * half], "zg", False) for k in range(2)]

    dq, dkv, grad_cum = attend(head_rows, head_kv, cum_gate[0])
    terms = exchange(dkv, GROUP)
    query_parts = exchange(dq, SP)
    *sums, part = call(
        group_sum_kernel,
        (*[shape((LANES, positions))] * zg, shape((dp, LANES, LANES))),
        me, terms, *near_rows,
    )
    own_sums = [sums[0]] + [shift(sums[k], "zg", zg, k) for k in range(1, zg)]
    grad_input = call(grad_input_kernel, shape((positions, features)), me, weight, *own_sums)
    parts = exchange(part, "dp")
    grad_queries = call(unpack_queries_kernel, shape((positions, features)), query_parts)
    along = call(sum_parts_kernel, shape((members, LANES, LANES)), parts)
    along = exchange(along, GROUP)
    along = call(sum_parts_kernel, shape((zg, LANES, LANES)), along)
    along = exchange(along, "zg")
    gradient = shape((LANES, kv_width), f32)
    grad_key, grad_value = call(finish_kernel, (gradient, gradient), along)
    return grad_input[None], grad_queries[None], grad_cum[None], grad_key, grad_value


def solution(mesh):
    sizes = {"heads": mesh.shape["sp"], "dp": mesh.shape["dp"], "zg": 4, "zp": 2, "xs": 4}
    split = Mesh(
        mesh.devices.reshape(sizes["zg"], sizes["zp"], sizes["xs"], sizes["dp"]),
        ("zg", "zp", "x", "dp"),
    )
    rows = P("dp", SP, None)
    weights = P("dp", None)
    return jax.shard_map(
        functools.partial(per_device, **sizes),
        mesh=split,
        in_specs=(rows, weights, weights, rows, rows, rows),
        out_specs=(rows, rows, rows, weights, weights),
        check_vma=False,
    )
```
